32 devices in a mesh: grp: 2 (over y), ep: 4 (over z), tp: 4 (over x, core).
Axes of the slice: x: 2, y: 2, z: 4, core: 2. Of those that a mesh axis runs over, the one named last changes fastest.
Arguments:
- out_gate: bfloat16 [1536, 4096], P(('grp', 'ep'), 'tp'), parts along dimension 0, may hold values from -6 to 6
- in_gate: bfloat16 [1536, 4096], P(('grp', 'ep'), 'tp'), parts along dimension 0, may hold values from -6 to 6
- values: bfloat16 [1536, 4096], P(('grp', 'ep'), 'tp'), parts along dimension 0, may hold values from -6 to 6
- conv_taps: float32 [3, 4096], P(None, 'tp'), may hold values from -3 to 3
- mixer_weight: bfloat16 [4096, 4096], P(None, 'tp'), may hold values from -0.09375 to 0.09375
- expert_input: bfloat16 [1536, 4096], P(('grp', 'ep', 'tp')), parts along dimension 0, may hold values from -6 to 6
- norm_gain: float32 [4096], replicated, may hold values from 0.1 to 1.9
- route_ids: int32 [1536, 2], P(('grp', 'ep')), parts along dimension 0, may hold values from 0 to 3, all different within a row; in each aligned block of 48 rows (0 to 47, 48 to 95, ...) at most 48 rows name the same one
- route_weights: float32 [1536, 2], P(('grp', 'ep')), parts along dimension 0, may hold values from 0.25 to 1.25
- gate_weight: bfloat16 [4, 4096, 1024], P('ep', None, 'tp'), may hold values from -0.09375 to 0.09375
- up_weight: bfloat16 [4, 4096, 1024], P('ep', None, 'tp'), may hold values from -0.09375 to 0.09375
- down_weight: bfloat16 [4, 1024, 4096], P('ep', None, 'tp'), may hold values from -0.1875 to 0.1875
- shared_gate: bfloat16 [4096, 512], P(None, 'tp'), may hold values from -0.09375 to 0.09375
- shared_up: bfloat16 [4096, 512], P(None, 'tp'), may hold values from -0.09375 to 0.09375
- shared_down: bfloat16 [512, 4096], P(None, 'tp'), may hold values from -0.25 to 0.25
Outputs:
- mixer_output: bfloat16 [1536, 4096], P(('grp', 'ep'), 'tp'), parts along dimension 0
- expert_output: bfloat16 [1536, 4096], P(('grp', 'ep'), 'tp'), parts along dimension 0
The draws below stay inside these ranges and needn't reach their ends.
There are 2 independent parts, one for each index of `grp`. The reference program is written for one: setup_inputs(seed, part) draws one part's arguments, and reference() takes and returns one part's arrays. A program takes and returns all parts, laid end to end along the dimension named above; an argument that names none is the same for every part. Nothing has to cross between parts.
Inputs may be any that keep to these rules, and one draw needn't show every extreme that they name: `route_ids`: the 2 entries of a row differ. In each aligned block of 48 rows (the routed tokens of one device) no expert is named by more than 48 rows, and in some block an expert is named by exactly 48 rows.
All inputs are finite; a program needn't handle non-finite values.
Results may differ from the reference program's by a relative error of at most 0.0067.
Values may be sent and summed in bfloat16 or wider, within the bound.
A program may use at most 64 MiB of HBM per device.

```python
import math
import jax
import jax.numpy as jnp
import numpy as np
from jax import lax

D = 4096
FF = 1024
SFF = 512
TOP_K = 2
TAPS = 3
TOKENS = 768
EXPERTS = 4
LANE_ROWS = 48
CAP = 48
N_EP = 4
N_TP = 4


def steps_of(key, shape, shards, least, top_value):
    gain, own = 1.0, jax.random.fold_in(key, 6)
    for dim, shards_of in shards:
        heights = jnp.exp(jax.random.uniform(jax.random.fold_in(own, dim), (shards_of,), jnp.float32, least / len(shards), top_value / len(shards)))
        gain = gain * jnp.repeat(heights, shape[dim] // shards_of).reshape([-1 if axis == dim else 1 for axis in range(len(shape))])
    return gain


def assign_block(stream_key, own, number, rows, number_of, top, bound, skew):
    ranking = jax.random.permutation(stream_key, number_of)
    heavy_load, ordinary = shares(number_of, rows * top, bound, skew, True), shares(number_of, rows * top, bound, skew, False)
    places = jnp.arange(number_of)

    def named(lengths, offset_by):
        used = int((lengths > 0).sum())
        fixed = max(1, used // 4)
        moved = fixed + (places - fixed + offset_by * (used - fixed)) % max(1, number_of - fixed)
        return jnp.zeros((number_of,), jnp.int32).at[ranking[jnp.where(places < fixed, places, moved)]].set(jnp.asarray(lengths, jnp.int32))

    lengths = jnp.where(number % 4 == 0, named(heavy_load, number // 4), named(ordinary, number - number // 4 - 1))
    mixed = jax.random.permutation(jax.random.fold_in(own, 3), number_of)
    giver, receiver = mixed[0:number_of // 2 * 2:2], mixed[1:number_of // 2 * 2:2]
    margin = jnp.minimum(lengths[giver] - 1, bound - lengths[receiver]) // 2
    margin = jnp.where((giver == ranking[0]) | (receiver == ranking[0]) | (lengths[receiver] == 0), 0, jnp.maximum(margin, 0))
    moved = jax.random.randint(jax.random.fold_in(own, 4), (number_of // 2,), 0, 1 << 20) % (margin + 1)
    lengths = lengths.at[giver].add(-moved).at[receiver].add(moved)
    labels = jnp.searchsorted(jnp.cumsum(lengths), jnp.arange(rows * top), side="right").astype(jnp.int32)
    listing = labels.reshape(top, rows).T
    listing = listing[jax.random.permutation(jax.random.fold_in(own, 1), rows)]
    offset_by = jax.random.randint(jax.random.fold_in(own, 2), (rows, 1), 0, top)
    return jnp.take_along_axis(listing, (jnp.arange(top)[None, :] + offset_by) % top, axis=1)


def shares(count, total, reach, lean, full):
    weights = [(1 << 20) // math.isqrt(grade ** lean) + 1 for grade in range(1, count + 1)]
    largest = reach if full else min(reach, max(-(-total // count), total * weights[0] // sum(weights)))
    least = 1 if total - largest >= count - 1 else 0
    counts, spare = [largest] + [least] * (count - 1), total - largest - least * (count - 1)
    while spare > 0:
        movable = [i for i in range(1, count) if counts[i] < largest] or [i for i in range(1, count) if counts[i] < reach]
        whole, budget = sum([weights[i] for i in movable]), spare
        for i in movable:
            extra = min(reach - counts[i], max(1, budget * weights[i] // whole), spare)
            counts[i] = counts[i] + extra
            spare = spare - extra
    return np.array(counts)


def bell_draw(key, extent, deviation, most, pieces=(), kind=jnp.bfloat16):
    values = deviation * jax.random.normal(key, extent, jnp.float32)
    if pieces:
        values = values * steps_of(key, extent, pieces, -0.22, 0.18)
    return jnp.clip(values, -most, most).astype(kind)


def setup_inputs(seed: int = 0, part: int = 0) -> dict:
    seeds = jax.random.split(jax.random.key(seed), 16)
    part_keys = jax.random.split(jax.random.fold_in(seeds[15], part), 16)
    out_gate = bell_draw(part_keys[0], (TOKENS, D), 1.0, 6.0, ((0, 4), (1, 4)))
    in_gate = bell_draw(part_keys[1], (TOKENS, D), 1.0, 6.0, ((0, 4), (1, 4)))
    values = bell_draw(part_keys[2], (TOKENS, D), 1.0, 6.0, ((0, 4), (1, 4)))
    conv_taps = bell_draw(seeds[3], (TAPS, D), 0.6, 3.0, ((1, 4),), jnp.float32)
    mixer_weight = bell_draw(seeds[4], (D, D), D ** -0.5, 0.09375, ((1, 4),))
    expert_input = bell_draw(part_keys[5], (TOKENS, D), 1.0, 6.0, ((0, 16),))
    norm_gain = jnp.clip(1.0 + 0.18 * jax.random.normal(seeds[6], (D,), jnp.float32), 0.1, 1.9)
    route_ids_keys = jax.random.split(jax.random.fold_in(part_keys[7], 1), TOKENS // LANE_ROWS)
    route_ids_turns = jax.random.permutation(jax.random.fold_in(part_keys[7], 3), TOKENS // LANE_ROWS)
    route_ids = jax.vmap(lambda own, number: assign_block(jax.random.fold_in(part_keys[7], 2), own, number, LANE_ROWS, EXPERTS, TOP_K, CAP, 2))(route_ids_keys, route_ids_turns).reshape((TOKENS, TOP_K))
    route_weights = jnp.clip(0.25 + 1.0 * jax.random.uniform(part_keys[8], (TOKENS, TOP_K), jnp.float32) ** steps_of(part_keys[8], (TOKENS, TOP_K), ((0, 4),), -0.2, 0.2), 0.25, 1.25)
    gate_weight = bell_draw(seeds[9], (EXPERTS, D, FF), D ** -0.5, 0.09375, ((0, 4), (2, 4)))
    up_weight = bell_draw(seeds[10], (EXPERTS, D, FF), D ** -0.5, 0.09375, ((0, 4), (2, 4)))
    down_weight = bell_draw(seeds[11], (EXPERTS, FF, D), FF ** -0.5, 0.1875, ((0, 4), (2, 4)))
    shared_gate = bell_draw(seeds[12], (D, SFF), D ** -0.5, 0.09375, ((1, 4),))
    shared_up = bell_draw(seeds[13], (D, SFF), D ** -0.5, 0.09375, ((1, 4),))
    shared_down = bell_draw(seeds[14], (SFF, D), SFF ** -0.5, 0.25, ((1, 4),))
    return dict(out_gate=out_gate, in_gate=in_gate, values=values, conv_taps=conv_taps, mixer_weight=mixer_weight, expert_input=expert_input, norm_gain=norm_gain, route_ids=route_ids, route_weights=route_weights, gate_weight=gate_weight, up_weight=up_weight, down_weight=down_weight, shared_gate=shared_gate, shared_up=shared_up, shared_down=shared_down)


norm_floor = 0.5

def layer_norm(tokens, norm_gain):
    widened = tokens.astype(jnp.float32)
    centred = widened - lax.optimization_barrier(jnp.mean(widened, axis=-1, keepdims=True))
    spread = lax.optimization_barrier(jnp.mean(centred * centred, axis=-1, keepdims=True))
    return (centred * lax.rsqrt(spread + norm_floor) * norm_gain).astype(jnp.bfloat16)

def expert_hidden(inputs, gate_part, up_part):
    gate_value = jnp.dot(inputs, gate_part, preferred_element_type=jnp.float32)
    up_value = jnp.dot(inputs, up_part, preferred_element_type=jnp.float32)
    return (jax.nn.silu(gate_value) * up_value).astype(jnp.bfloat16)

def reference(out_gate, in_gate, values, conv_taps, mixer_weight, expert_input, norm_gain, route_ids, route_weights, gate_weight, up_weight, down_weight, shared_gate, shared_up, shared_down):
    gated_values = (in_gate.astype(jnp.float32) * values.astype(jnp.float32)).astype(jnp.bfloat16)
    extended = jnp.concatenate([jnp.zeros((TAPS - 1, D), jnp.bfloat16), gated_values], axis=0).astype(jnp.float32)
    conv_state = conv_taps[0] * extended[:-2] + conv_taps[1] * extended[1:-1] + conv_taps[2] * extended[2:]
    mixed_rows = (out_gate.astype(jnp.float32) * conv_state).astype(jnp.bfloat16)
    mixer_output = jnp.dot(mixed_rows, mixer_weight, preferred_element_type=jnp.float32).astype(jnp.bfloat16)
    normed_rows = layer_norm(expert_input, norm_gain)
    buffer_len = N_EP * N_TP * CAP
    flat_ids = route_ids.reshape(-1).astype(jnp.int32)
    onehot = (flat_ids[:, None] == jnp.arange(EXPERTS, dtype=jnp.int32)[None, :]).astype(jnp.int32)
    slot_index = lax.optimization_barrier(jnp.sum((jnp.cumsum(onehot, axis=0) - onehot) * onehot, axis=1)).astype(jnp.int32)
    positions = flat_ids * buffer_len + slot_index
    owners = jnp.full((EXPERTS * buffer_len,), TOKENS, jnp.int32)
    owners = owners.at[positions].set(jnp.arange(TOKENS * TOP_K, dtype=jnp.int32) // TOP_K)

    def run_expert(operands):
        owner_rows, gate_part, up_part, down_part = operands
        picked = jnp.take(normed_rows, owner_rows, axis=0, mode='fill', fill_value=0)
        hidden = expert_hidden(picked, gate_part, up_part)
        return jnp.dot(hidden, down_part, preferred_element_type=jnp.float32).astype(jnp.bfloat16)
    results = lax.map(run_expert, (owners.reshape(EXPERTS, buffer_len), gate_weight, up_weight, down_weight))
    picked = jnp.take(results.reshape(EXPERTS * buffer_len, D), positions, axis=0).astype(jnp.float32)
    picked = picked.reshape(TOKENS, TOP_K, D)
    shared_hidden = expert_hidden(normed_rows, shared_gate, shared_up)
    shared_result = jnp.dot(shared_hidden, shared_down, preferred_element_type=jnp.float32)
    expert_output = (shared_result + lax.optimization_barrier(jnp.sum(route_weights[:, :, None] * picked, axis=1))).astype(jnp.bfloat16)
    return (mixer_output, expert_output)
```

```python
import functools

import jax
import jax.numpy as jnp
from jax import lax
from jax.experimental import pallas as pl
from jax.experimental.pallas import tpu as pltpu
from jax.sharding import PartitionSpec as P

MESH = pl.DeviceIdType.MESH
CORES = 2
TILE = 256

norm_floor = 0.5


def shifted(value, axis, steps):
    count = lax.axis_size(axis)
    leading, last = (max(0, -steps), min(count, count - steps))
    return lax.ppermute(value, axis, [(source, source + steps) for source in range(leading, last)])


def layer_norm(tokens, norm_gain):
    widened = tokens.astype(jnp.float32)
    centred = widened - jnp.mean(widened, axis=-1, keepdims=True)
    spread = jnp.mean(centred * centred, axis=-1, keepdims=True)
    return (centred * lax.rsqrt(spread + norm_floor) * norm_gain).astype(jnp.bfloat16)


def expert_hidden(inputs, gate_part, up_part):
    gate_value = jnp.dot(inputs, gate_part, preferred_element_type=jnp.float32)
    up_value = jnp.dot(inputs, up_part, preferred_element_type=jnp.float32)
    return (jax.nn.silu(gate_value) * up_value).astype(jnp.bfloat16)


def slot_ranks(route_ids, experts, lanes):
    tok_count, top_count = route_ids.shape
    grouped = route_ids.reshape(lanes, tok_count // lanes * top_count)
    onehot = (grouped[:, :, None] == jnp.arange(experts, dtype=jnp.int32)[None, None, :]).astype(
        jnp.int32
    )
    before = jnp.cumsum(onehot, axis=1) - onehot
    return jnp.sum(before * onehot, axis=2).reshape(tok_count, top_count)


def plain(
    out_gate,
    in_gate,
    values,
    conv_taps,
    mixer_weight,
    expert_input,
    norm_gain,
    route_ids,
    route_weights,
    gate_weight,
    up_weight,
    down_weight,
    shared_gate,
    shared_up,
    shared_down,
):
    experts = lax.axis_size("ep")
    lanes = lax.axis_size("tp")
    lane_rows = expert_input.shape[0]
    width = expert_input.shape[1]
    tok_count, top_count = route_ids.shape
    capacity = (2 * lane_rows * top_count + experts - 1) // experts
    gated_values = (in_gate.astype(jnp.float32) * values.astype(jnp.float32)).astype(jnp.bfloat16)
    previous = shifted(gated_values[-2:], "ep", 1)
    extended = jnp.concatenate([previous, gated_values], axis=0).astype(jnp.float32)
    conv_state = (
        conv_taps[0] * extended[:-2] + conv_taps[1] * extended[1:-1] + conv_taps[2] * extended[2:]
    )
    mixed_rows = (out_gate.astype(jnp.float32) * conv_state).astype(jnp.bfloat16)
    normed_own = layer_norm(expert_input, norm_gain)
    mixed_whole, normed_rows = (
        lax.all_gather(mixed_rows, "tp", axis=1, tiled=True),
        lax.all_gather(normed_own, "tp", axis=0, tiled=True),
    )
    mixer_output = jnp.dot(mixed_whole, mixer_weight, preferred_element_type=jnp.float32).astype(
        jnp.bfloat16
    )
    shared_part = expert_hidden(normed_rows, shared_gate, shared_up)
    slot_index = slot_ranks(route_ids, experts, lanes)
    lane_of_row = (jnp.arange(tok_count, dtype=jnp.int32) // lane_rows)[:, None]
    positions = (route_ids * lanes + lane_of_row) * capacity + slot_index
    lane_index = lax.axis_index("tp")
    lane_ids = lax.dynamic_slice_in_dim(route_ids, lane_index * lane_rows, lane_rows, 0)
    lane_slots = lax.dynamic_slice_in_dim(slot_index, lane_index * lane_rows, lane_rows, 0)
    lane_places = lane_ids * capacity + lane_slots
    local_rows = jnp.broadcast_to(jnp.arange(lane_rows, dtype=jnp.int32)[:, None], lane_ids.shape)
    owners = jnp.full((experts * capacity,), lane_rows, jnp.int32)
    owners = owners.at[lane_places.reshape(-1)].set(local_rows.reshape(-1))
    outgoing = jnp.take(normed_own, owners, axis=0, mode="fill", fill_value=0)
    arrived = lax.all_to_all(
        outgoing.reshape(experts, capacity, width), "ep", split_axis=0, concat_axis=0, tiled=True
    )
    segment = lax.all_gather(arrived[None], "tp", axis=0, tiled=True)
    hidden_rows = expert_hidden(segment.reshape(-1, width), gate_weight[0], up_weight[0])
    spread_hidden = hidden_rows.reshape(segment.shape[:-1] + (hidden_rows.shape[-1],))
    routed_hidden = jnp.swapaxes(spread_hidden, 0, 1).reshape(-1, spread_hidden.shape[-1])
    routed_whole, shared_whole = (
        lax.all_gather(routed_hidden, "tp", axis=1, tiled=True),
        lax.all_gather(shared_part, "tp", axis=1, tiled=True),
    )
    routed_result = jnp.dot(
        routed_whole, down_weight[0], preferred_element_type=jnp.float32
    ).astype(jnp.bfloat16)
    out_cols = routed_result.shape[-1]
    returned = lax.all_to_all(
        routed_result.reshape(experts, lanes * capacity, out_cols),
        "ep",
        split_axis=0,
        concat_axis=0,
        tiled=True,
    )
    shared_result = jnp.dot(shared_whole, shared_down, preferred_element_type=jnp.float32)
    picked = jnp.take(
        returned.reshape(experts * lanes * capacity, out_cols), positions.reshape(-1), axis=0
    )
    picked = picked.astype(jnp.float32).reshape(tok_count, top_count, out_cols)
    expert_output = (shared_result + jnp.sum(route_weights[:, :, None] * picked, axis=1)).astype(
        jnp.bfloat16
    )
    return (mixer_output, expert_output)


def silu_product(gate_value, up_value):
    return (gate_value * (1.0 / (1.0 + jnp.exp(-gate_value))) * up_value).astype(jnp.bfloat16)


def dot32(left, right):
    return jnp.dot(left, right, preferred_element_type=jnp.float32)


def kernel(
    n_ep,
    n_tp,
    ids,
    rw,
    og_h,
    ig_h,
    va_h,
    taps_h,
    mw_h,
    ei_h,
    ng_h,
    gw_h,
    uw_h,
    dw_h,
    sg_h,
    su_h,
    sd_h,
    mix_out,
    exp_out,
    og,
    ig,
    va,
    taps,
    mw,
    ei,
    ng,
    gw,
    uw,
    dw,
    sg,
    su,
    sd,
    tok,
    hid,
    shd,
    mixed,
    gated,
    halo,
    res,
    ret,
    ld,
    z_send,
    z_recv,
    x_send,
    x_recv,
    p_send,
    p_recv,
    r_send,
    r_recv,
    h_sem,
):
    e = lax.axis_index("ep")
    t = lax.axis_index("tp")
    n_x = n_tp // CORES
    partner = t + 1 - 2 * (t % CORES)
    lane_rows, width = ei.shape
    rows, chans = og.shape

    loads = {}
    for number, (name, src, dst) in enumerate(
        (
            ("ei", ei_h, ei),
            ("ng", ng_h, ng),
            ("ig", ig_h, ig),
            ("va", va_h, va),
            ("og", og_h, og),
            ("taps", taps_h, taps),
            ("gw", gw_h, gw),
            ("uw", uw_h, uw),
            ("sg", sg_h, sg),
            ("su", su_h, su),
            ("dw", dw_h, dw),
            ("sd", sd_h, sd),
            ("mw", mw_h, mw),
        )
    ):
        loads[name] = pltpu.make_async_copy(src, dst, ld.at[number])
        loads[name].start()

    barrier = pltpu.get_barrier_semaphore()
    greeted = [{"ep": (e + d) % n_ep, "tp": t} for d in range(1, n_ep)]
    greeted += [{"ep": e, "tp": (t + CORES * d) % n_tp} for d in range(1, n_x)]
    greeted += [{"ep": e, "tp": partner}]
    for peer in greeted:
        pl.semaphore_signal(barrier, inc=1, device_id=peer, device_id_type=MESH)

    def remote(src, dst, send, recv, ep, tp):
        return pltpu.make_async_remote_copy(
            src_ref=src,
            dst_ref=dst,
            send_sem=send,
            recv_sem=recv,
            device_id={"ep": ep, "tp": tp},
            device_id_type=MESH,
        )

    def cross(slot, g, d, lane):
        return remote(
            slot(lane), slot(lane), x_send.at[g, d - 1], x_recv.at[g, d - 1],
            e, (t + CORES * d) % n_tp,
        )

    def across(slot, g, d, lane):
        return remote(slot(lane), slot(lane), p_send.at[g, d], p_recv.at[g, d], e, partner)

    def from_x(d):
        return (t + n_tp - CORES * d) % n_tp

    def from_partner(d):
        return (partner + n_tp - CORES * d) % n_tp

    def gather_start(slot, g):
        for d in range(1, n_x):
            cross(slot, g, d, t).start()
        across(slot, g, 0, t).start()

    def gather_forward(slot, g):
        for d in range(1, n_x):
            cross(slot, g, d, from_x(d)).wait_recv()
            across(slot, g, d, from_x(d)).start()

    def gather_finish(slot, g):
        for d in range(n_x):
            across(slot, g, d, from_partner(d)).wait_recv()

    def gather_drain(slot, g):
        for d in range(1, n_x):
            cross(slot, g, d, t).wait_send()
            across(slot, g, d, from_x(d)).wait_send()
        across(slot, g, 0, t).wait_send()

    shared_g, mixed_g = 2 * n_ep, 2 * n_ep + 1

    def tok_slot(j):
        return lambda lane: tok.at[j, lane]

    def hid_slot(j):
        return lambda lane: hid.at[j, lane]

    def shd_slot(lane):
        return shd.at[lane]

    def mixed_slot(lane):
        return mixed.at[lane]

    nearest = jnp.minimum(e, n_ep - 1 - e)
    left_short = e <= n_ep - 1 - e

    def block_at(k):
        near = jnp.where(k % 2 == 1, e - (k + 1) // 2, e + k // 2)
        far = jnp.where(left_short, k, n_ep - 1 - k)
        return jnp.where(k <= 2 * nearest, near, far)

    def z_right(j):
        return remote(tok.at[j, t], tok.at[j, t], z_send.at[0, j], z_recv.at[j],
                      jnp.minimum(e + 1, n_ep - 1), t)

    def z_left(j):
        return remote(tok.at[j, t], tok.at[j, t], z_send.at[1, j], z_recv.at[j],
                      jnp.maximum(e - 1, 0), t)

    def goes_right(j):
        return (j <= e) & (e < n_ep - 1)

    def goes_left(j):
        return (j >= e) & (e > 0)

    def spread(k):
        j = block_at(k)

        @pl.when(k > 0)
        def _():
            z_right(j).wait_recv()

        @pl.when(goes_right(j))
        def _():
            z_right(j).start()

        @pl.when(goes_left(j))
        def _():
            z_left(j).start()

        gather_start(tok_slot(j), j)

    def back(j):
        return remote(res.at[j], ret.at[e], r_send.at[j], r_recv.at[e], j, t)

    loads["ei"].wait()
    loads["ng"].wait()

    def norm_rows(r, _):
        at = pl.ds(pl.multiple_of(r * 16, 16), 16)
        widened = ei[at, :].astype(jnp.float32)
        centred = widened - jnp.mean(widened, axis=-1, keepdims=True)
        spread_of = jnp.mean(centred * centred, axis=-1, keepdims=True)
        normed = centred * lax.rsqrt(spread_of + norm_floor) * ng[...]
        tok[e, t, at, :] = normed.astype(jnp.bfloat16)
        return 0

    lax.fori_loop(0, lane_rows // 16, norm_rows, 0)
    pl.semaphore_wait(barrier, len(greeted))
    spread(0)

    loads["ig"].wait()
    loads["va"].wait()

    def gate_cols(c, _):
        at = pl.ds(pl.multiple_of(c * 128, 128), 128)
        gated[:, at] = (ig[:, at].astype(jnp.float32) * va[:, at].astype(jnp.float32)).astype(
            jnp.bfloat16
        )
        return 0

    lax.fori_loop(0, chans // 128, gate_cols, 0)

    def halo_copy():
        return remote(gated.at[pl.ds(rows - 16, 16)], halo, h_sem.at[0], h_sem.at[1],
                      jnp.minimum(e + 1, n_ep - 1), t)

    @pl.when(e < n_ep - 1)
    def _():
        halo_copy().start()

    loads["og"].wait()
    loads["taps"].wait()

    @pl.when(e == 0)
    def _():
        halo[...] = jnp.zeros_like(halo)

    @pl.when(e > 0)
    def _():
        halo_copy().wait_recv()

    def mix_cols(c, _):
        at = pl.ds(pl.multiple_of(c * 128, 128), 128)
        now = gated[:, at].astype(jnp.float32)
        before = halo[:, at].astype(jnp.float32)
        place = lax.broadcasted_iota(jnp.int32, now.shape, 0)
        one = jnp.where(place == 0, before[15:16], pltpu.roll(now, 1, 0))
        two = jnp.where(
            place == 0, before[14:15], jnp.where(place == 1, before[15:16], pltpu.roll(now, 2, 0))
        )
        state = taps[0:1, at] * two + taps[1:2, at] * one + taps[2:3, at] * now
        mixed[t, :, at] = (og[:, at].astype(jnp.float32) * state).astype(jnp.bfloat16)
        return 0

    lax.fori_loop(0, chans // 128, mix_cols, 0)
    for name in ("gw", "uw", "sg", "su"):
        loads[name].wait()

    def step(s, _):
        @pl.when(s + 1 < n_ep)
        def _():
            spread(s + 1)

        @pl.when(s < n_ep)
        def _():
            j = block_at(s)
            gather_forward(tok_slot(j), j)
            gather_finish(tok_slot(j), j)
            block = tok[j].reshape(rows, width)
            hid[j, t] = silu_product(dot32(block, gw[...]), dot32(block, uw[...]))
            gather_start(hid_slot(j), n_ep + j)

        @pl.when(s == 0)
        def _():
            block = tok[e].reshape(rows, width)
            shd[t] = silu_product(dot32(block, sg[...]), dot32(block, su[...]))
            gather_start(shd_slot, shared_g)
            loads["dw"].wait()

        @pl.when(s == n_ep - 1)
        def _():
            gather_start(mixed_slot, mixed_g)

        @pl.when(s >= 1)
        def _():
            j = block_at(s - 1)
            gather_forward(hid_slot(j), n_ep + j)
            gather_finish(hid_slot(j), n_ep + j)
            part = hid.shape[-1]
            for c in range(chans // TILE):
                at = slice(c * TILE, (c + 1) * TILE)
                total = dot32(hid[j, 0], dw[0:part, at])
                for lane in range(1, n_tp):
                    total += dot32(hid[j, lane], dw[lane * part : (lane + 1) * part, at])
                res[j, :, at] = total.astype(jnp.bfloat16)

            @pl.when(j != e)
            def _():
                back(j).start()

        return 0

    lax.fori_loop(0, n_ep + 1, step, 0)

    gather_forward(shd_slot, shared_g)
    gather_forward(mixed_slot, mixed_g)
    gather_finish(shd_slot, shared_g)
    loads["sd"].wait()
    loads["mw"].wait()
    gather_finish(mixed_slot, mixed_g)

    def mixer_cols(c, _):
        at = pl.ds(pl.multiple_of(c * TILE, TILE), TILE)
        total = dot32(mixed[0], mw[0:chans, at])
        for lane in range(1, n_tp):
            total += dot32(mixed[lane], mw[lane * chans : (lane + 1) * chans, at])
        mix_out[:, at] = total.astype(jnp.bfloat16)
        return 0

    lax.fori_loop(0, chans // TILE, mixer_cols, 0)

    for d in range(1, n_ep):
        i = (e + d) % n_ep
        remote(res.at[i], ret.at[i], r_send.at[i], r_recv.at[i], i, t).wait_recv()

    def combine_cols(c, _):
        at = pl.ds(pl.multiple_of(c * TILE, TILE), TILE)
        part = shd.shape[-1]
        total = dot32(shd[0], sd[0:part, at])
        for lane in range(1, n_tp):
            total += dot32(shd[lane], sd[lane * part : (lane + 1) * part, at])
        for d in range(n_ep):
            i = (e + d) % n_ep
            weight = jnp.sum(jnp.where(ids[...] == i, rw[...], 0.0), axis=1, keepdims=True)
            found = res[e, :, at] if d == 0 else ret[i, :, at]
            total += weight * found.astype(jnp.float32)
        exp_out[:, at] = total.astype(jnp.bfloat16)
        return 0

    lax.fori_loop(0, chans // TILE, combine_cols, 0)

    @pl.when(e < n_ep - 1)
    def _():
        halo_copy().wait_send()

    def drain(j, _):
        @pl.when(goes_right(j))
        def _():
            z_right(j).wait_send()

        @pl.when(goes_left(j))
        def _():
            z_left(j).wait_send()

        gather_drain(tok_slot(j), j)
        gather_drain(hid_slot(j), n_ep + j)

        @pl.when(j != e)
        def _():
            back(j).wait_send()

        return 0

    lax.fori_loop(0, n_ep, drain, 0)
    gather_drain(shd_slot, shared_g)
    gather_drain(mixed_slot, mixed_g)


def joined(n_ep, n_tp, *args):
    (og, ig, va, taps, mw, ei, ng, ids, rw, gw, uw, dw, sg, su, sd) = args
    gw, uw, dw, ng = gw[0], uw[0], dw[0], ng[None]
    bf, f32 = jnp.bfloat16, jnp.float32
    rows, chans = og.shape
    lane_rows, width = ei.shape
    n_x = n_tp // CORES
    sems = 2 * n_ep + 2
    big = (og, ig, va, taps, mw, ei, ng, gw, uw, dw, sg, su, sd)
    out = jax.ShapeDtypeStruct((rows, chans), bf)
    vmem = pl.BlockSpec(memory_space=pltpu.VMEM)
    dma = pltpu.SemaphoreType.DMA
    return pl.pallas_call(
        functools.partial(kernel, n_ep, n_tp),
        out_shape=(out, out),
        in_specs=[vmem, vmem] + [pl.BlockSpec(memory_space=pl.ANY)] * len(big),
        out_specs=(vmem, vmem),
        scratch_shapes=[pltpu.VMEM(a.shape, a.dtype) for a in big]
        + [
            pltpu.VMEM((n_ep, n_tp, lane_rows, width), bf),
            pltpu.VMEM((n_ep, n_tp, rows, gw.shape[-1]), bf),
            pltpu.VMEM((n_tp, rows, sg.shape[-1]), bf),
            pltpu.VMEM((n_tp, rows, chans), bf),
            pltpu.VMEM((rows, chans), bf),
            pltpu.VMEM((16, chans), bf),
            pltpu.VMEM((n_ep, rows, chans), bf),
            pltpu.VMEM((n_ep, rows, chans), bf),
            dma((len(big),)),
            dma((2, n_ep)),
            dma((n_ep,)),
            dma((sems, max(1, n_x - 1))),
            dma((sems, max(1, n_x - 1))),
            dma((sems, n_x)),
            dma((sems, n_x)),
            dma((n_ep,)),
            dma((n_ep,)),
            dma((2,)),
        ],
        compiler_params=pltpu.CompilerParams(
            collective_id=0, has_side_effects=True, vmem_limit_bytes=60 * 1024 * 1024
        ),
    )(ids, rw, *big)


def local(*args):
    n_ep, n_tp = lax.axis_size("ep"), lax.axis_size("tp")
    chans, lane_rows = args[0].shape[1], args[5].shape[0]
    aligned = (
        n_tp % CORES == 0
        and lane_rows % 16 == 0
        and lane_rows * n_tp == args[0].shape[0]
        and chans % TILE == 0
        and args[9].shape[2] % 128 == 0
        and args[12].shape[1] % 128 == 0
    )
    return joined(n_ep, n_tp, *args) if aligned else plain(*args)


def solution(mesh):
    placed = (
        P(("grp", "ep"), "tp"),
        P(("grp", "ep"), "tp"),
        P(("grp", "ep"), "tp"),
        P(None, "tp"),
        P(None, "tp"),
        P(("grp", "ep", "tp"), None),
        P(),
        P(("grp", "ep"), None),
        P(("grp", "ep"), None),
        P("ep", None, "tp"),
        P("ep", None, "tp"),
        P("ep", None, "tp"),
        P(None, "tp"),
        P(None, "tp"),
        P(None, "tp"),
    )
    return jax.shard_map(
        local,
        mesh=mesh,
        in_specs=placed,
        out_specs=(P(("grp", "ep"), "tp"), P(("grp", "ep"), "tp")),
        check_vma=False,
    )
```

```python
import functools

import jax
import jax.numpy as jnp
from jax import lax
from jax.experimental import pallas as pl
from jax.experimental.pallas import tpu as pltpu
from jax.sharding import PartitionSpec as P

MESH = pl.DeviceIdType.MESH
CORES = 2
TILE = 256
CHUNKS = 4

norm_floor = 0.5


def shifted(value, axis, steps):
    count = lax.axis_size(axis)
    leading, last = (max(0, -steps), min(count, count - steps))
    return lax.ppermute(value, axis, [(source, source + steps) for source in range(leading, last)])


def layer_norm(tokens, norm_gain):
    widened = tokens.astype(jnp.float32)
    centred = widened - jnp.mean(widened, axis=-1, keepdims=True)
    spread = jnp.mean(centred * centred, axis=-1, keepdims=True)
    return (centred * lax.rsqrt(spread + norm_floor) * norm_gain).astype(jnp.bfloat16)


def expert_hidden(inputs, gate_part, up_part):
    gate_value = jnp.dot(inputs, gate_part, preferred_element_type=jnp.float32)
    up_value = jnp.dot(inputs, up_part, preferred_element_type=jnp.float32)
    return (jax.nn.silu(gate_value) * up_value).astype(jnp.bfloat16)


def slot_ranks(route_ids, experts, lanes):
    tok_count, top_count = route_ids.shape
    grouped = route_ids.reshape(lanes, tok_count // lanes * top_count)
    onehot = (grouped[:, :, None] == jnp.arange(experts, dtype=jnp.int32)[None, None, :]).astype(
        jnp.int32
    )
    before = jnp.cumsum(onehot, axis=1) - onehot
    return jnp.sum(before * onehot, axis=2).reshape(tok_count, top_count)


def plain(
    out_gate,
    in_gate,
    values,
    conv_taps,
    mixer_weight,
    expert_input,
    norm_gain,
    route_ids,
    route_weights,
    gate_weight,
    up_weight,
    down_weight,
    shared_gate,
    shared_up,
    shared_down,
):
    experts = lax.axis_size("ep")
    lanes = lax.axis_size("tp")
    lane_rows = expert_input.shape[0]
    width = expert_input.shape[1]
    tok_count, top_count = route_ids.shape
    capacity = (2 * lane_rows * top_count + experts - 1) // experts
    gated_values = (in_gate.astype(jnp.float32) * values.astype(jnp.float32)).astype(jnp.bfloat16)
    previous = shifted(gated_values[-2:], "ep", 1)
    extended = jnp.concatenate([previous, gated_values], axis=0).astype(jnp.float32)
    conv_state = (
        conv_taps[0] * extended[:-2] + conv_taps[1] * extended[1:-1] + conv_taps[2] * extended[2:]
    )
    mixed_rows = (out_gate.astype(jnp.float32) * conv_state).astype(jnp.bfloat16)
    normed_own = layer_norm(expert_input, norm_gain)
    mixed_whole, normed_rows = (
        lax.all_gather(mixed_rows, "tp", axis=1, tiled=True),
        lax.all_gather(normed_own, "tp", axis=0, tiled=True),
    )
    mixer_output = jnp.dot(mixed_whole, mixer_weight, preferred_element_type=jnp.float32).astype(
        jnp.bfloat16
    )
    shared_part = expert_hidden(normed_rows, shared_gate, shared_up)
    slot_index = slot_ranks(route_ids, experts, lanes)
    lane_of_row = (jnp.arange(tok_count, dtype=jnp.int32) // lane_rows)[:, None]
    positions = (route_ids * lanes + lane_of_row) * capacity + slot_index
    lane_index = lax.axis_index("tp")
    lane_ids = lax.dynamic_slice_in_dim(route_ids, lane_index * lane_rows, lane_rows, 0)
    lane_slots = lax.dynamic_slice_in_dim(slot_index, lane_index * lane_rows, lane_rows, 0)
    lane_places = lane_ids * capacity + lane_slots
    local_rows = jnp.broadcast_to(jnp.arange(lane_rows, dtype=jnp.int32)[:, None], lane_ids.shape)
    owners = jnp.full((experts * capacity,), lane_rows, jnp.int32)
    owners = owners.at[lane_places.reshape(-1)].set(local_rows.reshape(-1))
    outgoing = jnp.take(normed_own, owners, axis=0, mode="fill", fill_value=0)
    arrived = lax.all_to_all(
        outgoing.reshape(experts, capacity, width), "ep", split_axis=0, concat_axis=0, tiled=True
    )
    segment = lax.all_gather(arrived[None], "tp", axis=0, tiled=True)
    hidden_rows = expert_hidden(segment.reshape(-1, width), gate_weight[0], up_weight[0])
    spread_hidden = hidden_rows.reshape(segment.shape[:-1] + (hidden_rows.shape[-1],))
    routed_hidden = jnp.swapaxes(spread_hidden, 0, 1).reshape(-1, spread_hidden.shape[-1])
    routed_whole, shared_whole = (
        lax.all_gather(routed_hidden, "tp", axis=1, tiled=True),
        lax.all_gather(shared_part, "tp", axis=1, tiled=True),
    )
    routed_result = jnp.dot(
        routed_whole, down_weight[0], preferred_element_type=jnp.float32
    ).astype(jnp.bfloat16)
    out_cols = routed_result.shape[-1]
    returned = lax.all_to_all(
        routed_result.reshape(experts, lanes * capacity, out_cols),
        "ep",
        split_axis=0,
        concat_axis=0,
        tiled=True,
    )
    shared_result = jnp.dot(shared_whole, shared_down, preferred_element_type=jnp.float32)
    picked = jnp.take(
        returned.reshape(experts * lanes * capacity, out_cols), positions.reshape(-1), axis=0
    )
    picked = picked.astype(jnp.float32).reshape(tok_count, top_count, out_cols)
    expert_output = (shared_result + jnp.sum(route_weights[:, :, None] * picked, axis=1)).astype(
        jnp.bfloat16
    )
    return (mixer_output, expert_output)


def silu_product(gate_value, up_value):
    return (gate_value * (1.0 / (1.0 + jnp.exp(-gate_value))) * up_value).astype(jnp.bfloat16)


def dot32(left, right):
    return jnp.dot(left, right, preferred_element_type=jnp.float32)


def kernel(
    n_ep,
    n_tp,
    ids,
    rw,
    og_h,
    ig_h,
    va_h,
    taps_h,
    mw_h,
    ei_h,
    ng_h,
    gw_h,
    uw_h,
    dw_h,
    sg_h,
    su_h,
    sd_h,
    mix_out,
    exp_out,
    og,
    ig,
    va,
    taps,
    mw,
    ei,
    ng,
    gw,
    uw,
    dw,
    sg,
    su,
    sd,
    tok,
    hid,
    shd,
    mixed,
    gated,
    halo,
    res,
    pin,
    wts,
    ld,
    z_send,
    z_recv,
    x_send,
    x_recv,
    p_send,
    p_recv,
    r_send,
    r_recv,
    w_send,
    w_recv,
    h_sem,
):
    e = lax.axis_index("ep")
    t = lax.axis_index("tp")
    n_x = n_tp // CORES
    partner = t + 1 - 2 * (t % CORES)
    lane_rows, width = ei.shape
    rows, chans = og.shape

    loads = {}
    for number, (name, src, dst) in enumerate(
        (
            ("ei", ei_h, ei),
            ("ng", ng_h, ng),
            ("ig", ig_h, ig),
            ("va", va_h, va),
            ("og", og_h, og),
            ("taps", taps_h, taps),
            ("gw", gw_h, gw),
            ("uw", uw_h, uw),
            ("sg", sg_h, sg),
            ("su", su_h, su),
            ("dw", dw_h, dw),
            ("sd", sd_h, sd),
            ("mw", mw_h, mw),
        )
    ):
        loads[name] = pltpu.make_async_copy(src, dst, ld.at[number])
        loads[name].start()

    barrier = pltpu.get_barrier_semaphore()
    greeted = [{"ep": (e + d) % n_ep, "tp": t} for d in range(1, n_ep)]
    greeted += [{"ep": e, "tp": (t + CORES * d) % n_tp} for d in range(1, n_x)]
    greeted += [{"ep": e, "tp": partner}]
    for peer in greeted:
        pl.semaphore_signal(barrier, inc=1, device_id=peer, device_id_type=MESH)

    def remote(src, dst, send, recv, ep, tp):
        return pltpu.make_async_remote_copy(
            src_ref=src,
            dst_ref=dst,
            send_sem=send,
            recv_sem=recv,
            device_id={"ep": ep, "tp": tp},
            device_id_type=MESH,
        )

    def cross(slot, g, d, lane):
        return remote(
            slot(lane), slot(lane), x_send.at[g, d - 1], x_recv.at[g, d - 1],
            e, (t + CORES * d) % n_tp,
        )

    def across(slot, g, d, lane):
        return remote(slot(lane), slot(lane), p_send.at[g, d], p_recv.at[g, d], e, partner)

    def from_x(d):
        return (t + n_tp - CORES * d) % n_tp

    def from_partner(d):
        return (partner + n_tp - CORES * d) % n_tp

    def gather_start(slot, g):
        for d in range(1, n_x):
            cross(slot, g, d, t).start()
        across(slot, g, 0, t).start()

    def gather_forward(slot, g):
        for d in range(1, n_x):
            cross(slot, g, d, from_x(d)).wait_recv()
            across(slot, g, d, from_x(d)).start()

    def gather_finish(slot, g):
        for d in range(n_x):
            across(slot, g, d, from_partner(d)).wait_recv()

    def gather_drain(slot, g):
        for d in range(1, n_x):
            cross(slot, g, d, t).wait_send()
            across(slot, g, d, from_x(d)).wait_send()
        across(slot, g, 0, t).wait_send()

    shared_g, mixed_g = 2 * n_ep, 2 * n_ep + 1

    def tok_slot(j):
        return lambda lane: tok.at[j, lane]

    def hid_slot(j):
        return lambda lane: hid.at[j, lane]

    def shd_slot(lane):
        return shd.at[lane]

    def mixed_slot(lane):
        return mixed.at[lane]

    nearest = jnp.minimum(e, n_ep - 1 - e)
    left_short = e <= n_ep - 1 - e

    def block_at(k):
        near = jnp.where(k % 2 == 1, e - (k + 1) // 2, e + k // 2)
        far = jnp.where(left_short, k, n_ep - 1 - k)
        return jnp.where(k <= 2 * nearest, near, far)

    def z_right(j):
        return remote(tok.at[j, t], tok.at[j, t], z_send.at[0, j], z_recv.at[j],
                      jnp.minimum(e + 1, n_ep - 1), t)

    def z_left(j):
        return remote(tok.at[j, t], tok.at[j, t], z_send.at[1, j], z_recv.at[j],
                      jnp.maximum(e - 1, 0), t)

    def goes_right(j):
        return (j <= e) & (e < n_ep - 1)

    def goes_left(j):
        return (j >= e) & (e > 0)

    def spread(k):
        j = block_at(k)

        @pl.when(k > 0)
        def _():
            z_right(j).wait_recv()

        @pl.when(goes_right(j))
        def _():
            z_right(j).start()

        @pl.when(goes_left(j))
        def _():
            z_left(j).start()

        gather_start(tok_slot(j), j)

    piece = rows // CHUNKS

    def hop(j, c):
        at = pl.ds(pl.multiple_of(c * piece, 16), piece)
        after = jnp.clip(jnp.where(j > e, e + 1, e - 1), 0, n_ep - 1)
        slot = jnp.where((j < e) & (after == j), n_ep, j)
        return remote(res.at[j, at], pin.at[slot, at], r_send.at[j, c], r_recv.at[slot, c], after, t)

    def hop_arrives(slot, c):
        at = pl.ds(pl.multiple_of(c * piece, 16), piece)
        remote(res.at[0, at], pin.at[slot, at], r_send.at[0, c], r_recv.at[slot, c],
               jnp.clip(e + 1, 0, n_ep - 1), t).wait_recv()

    inner = (e > 0) & (e < n_ep - 1)

    def weights_to(d):
        return remote(wts.at[e], wts.at[e], w_send.at[d - 1], w_recv.at[e], (e + d) % n_ep, t)

    def weight_column(j):
        held = wts[j]
        mine = jnp.where(lax.broadcasted_iota(jnp.int32, held.shape, 0) == e, held, 0.0)
        line = jnp.sum(mine, axis=0, keepdims=True)
        shape = (rows, held.shape[1])
        same = lax.broadcasted_iota(jnp.int32, shape, 0) == lax.broadcasted_iota(jnp.int32, shape, 1)
        return jnp.sum(jnp.where(same, line, 0.0), axis=1, keepdims=True)

    loads["ei"].wait()
    loads["ng"].wait()

    def norm_rows(r, _):
        at = pl.ds(pl.multiple_of(r * 16, 16), 16)
        widened = ei[at, :].astype(jnp.float32)
        centred = widened - jnp.mean(widened, axis=-1, keepdims=True)
        spread_of = jnp.mean(centred * centred, axis=-1, keepdims=True)
        normed = centred * lax.rsqrt(spread_of + norm_floor) * ng[...]
        tok[e, t, at, :] = normed.astype(jnp.bfloat16)
        return 0

    lax.fori_loop(0, lane_rows // 16, norm_rows, 0)
    pl.semaphore_wait(barrier, len(greeted))
    spread(0)

    place = lax.broadcasted_iota(jnp.int32, (wts.shape[1], rows), 0)
    dense = jnp.zeros(place.shape, jnp.float32)
    for k in range(ids.shape[0]):
        dense += jnp.where(ids[k : k + 1, :] == place, rw[k : k + 1, :], 0.0)
    wts[e] = jnp.zeros(wts.shape[1:], jnp.float32)
    wts[e, :, 0:rows] = dense
    for d in range(1, n_ep):
        weights_to(d).start()

    loads["ig"].wait()
    loads["va"].wait()

    def gate_cols(c, _):
        at = pl.ds(pl.multiple_of(c * 128, 128), 128)
        gated[:, at] = (ig[:, at].astype(jnp.float32) * va[:, at].astype(jnp.float32)).astype(
            jnp.bfloat16
        )
        return 0

    lax.fori_loop(0, chans // 128, gate_cols, 0)

    def halo_copy():
        return remote(gated.at[pl.ds(rows - 16, 16)], halo, h_sem.at[0], h_sem.at[1],
                      jnp.minimum(e + 1, n_ep - 1), t)

    @pl.when(e < n_ep - 1)
    def _():
        halo_copy().start()

    loads["og"].wait()
    loads["taps"].wait()

    @pl.when(e == 0)
    def _():
        halo[...] = jnp.zeros_like(halo)

    @pl.when(e > 0)
    def _():
        halo_copy().wait_recv()

    def mix_cols(c, _):
        at = pl.ds(pl.multiple_of(c * 128, 128), 128)
        now = gated[:, at].astype(jnp.float32)
        before = halo[:, at].astype(jnp.float32)
        place = lax.broadcasted_iota(jnp.int32, now.shape, 0)
        one = jnp.where(place == 0, before[15:16], pltpu.roll(now, 1, 0))
        two = jnp.where(
            place == 0, before[14:15], jnp.where(place == 1, before[15:16], pltpu.roll(now, 2, 0))
        )
        state = taps[0:1, at] * two + taps[1:2, at] * one + taps[2:3, at] * now
        mixed[t, :, at] = (og[:, at].astype(jnp.float32) * state).astype(jnp.bfloat16)
        return 0

    lax.fori_loop(0, chans // 128, mix_cols, 0)
    for name in ("gw", "uw", "sg", "su"):
        loads[name].wait()

    def step(s, _):
        @pl.when(s + 1 < n_ep)
        def _():
            spread(s + 1)

        @pl.when(s < n_ep)
        def _():
            j = block_at(s)
            gather_forward(tok_slot(j), j)
            gather_finish(tok_slot(j), j)
            block = tok[j].reshape(rows, width)
            hid[j, t] = silu_product(dot32(block, gw[...]), dot32(block, uw[...]))
            gather_start(hid_slot(j), n_ep + j)

        @pl.when(s == 0)
        def _():
            block = tok[e].reshape(rows, width)
            shd[t] = silu_product(dot32(block, sg[...]), dot32(block, su[...]))
            gather_start(shd_slot, shared_g)
            loads["dw"].wait()

        @pl.when(s == n_ep - 1)
        def _():
            gather_start(mixed_slot, mixed_g)

        @pl.when(s >= 1)
        def _():
            j = block_at(s - 1)
            gather_forward(hid_slot(j), n_ep + j)
            gather_finish(hid_slot(j), n_ep + j)
            part = hid.shape[-1]

            @pl.when(j != e)
            def _():
                remote(wts.at[e], wts.at[j], w_send.at[0], w_recv.at[j], j, t).wait_recv()

            weight = weight_column(j)
            for c in range(chans // TILE):
                at = slice(c * TILE, (c + 1) * TILE)
                total = dot32(hid[j, 0], dw[0:part, at])
                for lane in range(1, n_tp):
                    total += dot32(hid[j, lane], dw[lane * part : (lane + 1) * part, at])
                res[j, :, at] = (weight * total).astype(jnp.bfloat16)

            @pl.when((j != e) & ~inner)
            def _():
                for c in range(CHUNKS):
                    hop(j, c).start()

        return 0

    lax.fori_loop(0, n_ep + 1, step, 0)

    gather_forward(shd_slot, shared_g)

    for phase in range(2):
        right = left_short if phase == 0 else ~left_short

        def relay(d, _):
            j = jnp.where(right, e + d, e - d)

            @pl.when(inner & (j >= 0) & (j < n_ep))
            def _():
                def relay_piece(c, _):
                    at = pl.ds(pl.multiple_of(c * piece, 16), piece)
                    hop_arrives(j, c)
                    total = res[j, at, :].astype(jnp.float32) + pin[j, at, :].astype(jnp.float32)
                    res[j, at, :] = total.astype(jnp.bfloat16)
                    hop(j, c).start()
                    return 0

                lax.fori_loop(0, CHUNKS, relay_piece, 0)

            return 0

        lax.fori_loop(1, n_ep, relay, 0)

    gather_forward(mixed_slot, mixed_g)
    gather_finish(shd_slot, shared_g)
    loads["sd"].wait()
    loads["mw"].wait()
    gather_finish(mixed_slot, mixed_g)

    def mixer_cols(c, _):
        at = pl.ds(pl.multiple_of(c * TILE, TILE), TILE)
        total = dot32(mixed[0], mw[0:chans, at])
        for lane in range(1, n_tp):
            total += dot32(mixed[lane], mw[lane * chans : (lane + 1) * chans, at])
        mix_out[:, at] = total.astype(jnp.bfloat16)
        return 0

    lax.fori_loop(0, chans // TILE, mixer_cols, 0)

    for here, slot in ((e > 0, e), (e < n_ep - 1, n_ep)):

        @pl.when(here)
        def _():
            for c in range(CHUNKS):
                hop_arrives(slot, c)

        @pl.when(~here)
        def _():
            pin[slot] = jnp.zeros(pin.shape[1:], pin.dtype)

    def combine_cols(c, _):
        at = pl.ds(pl.multiple_of(c * TILE, TILE), TILE)
        part = shd.shape[-1]
        total = dot32(shd[0], sd[0:part, at])
        for lane in range(1, n_tp):
            total += dot32(shd[lane], sd[lane * part : (lane + 1) * part, at])
        for found in (res[e, :, at], pin[e, :, at], pin[n_ep, :, at]):
            total += found.astype(jnp.float32)
        exp_out[:, at] = total.astype(jnp.bfloat16)
        return 0

    lax.fori_loop(0, chans // TILE, combine_cols, 0)

    @pl.when(e < n_ep - 1)
    def _():
        halo_copy().wait_send()

    def drain(j, _):
        @pl.when(goes_right(j))
        def _():
            z_right(j).wait_send()

        @pl.when(goes_left(j))
        def _():
            z_left(j).wait_send()

        gather_drain(tok_slot(j), j)
        gather_drain(hid_slot(j), n_ep + j)

        @pl.when(j != e)
        def _():
            for c in range(CHUNKS):
                hop(j, c).wait_send()

        return 0

    lax.fori_loop(0, n_ep, drain, 0)
    for d in range(1, n_ep):
        weights_to(d).wait_send()
    gather_drain(shd_slot, shared_g)
    gather_drain(mixed_slot, mixed_g)


def joined(n_ep, n_tp, *args):
    (og, ig, va, taps, mw, ei, ng, ids, rw, gw, uw, dw, sg, su, sd) = args
    gw, uw, dw, ng = gw[0], uw[0], dw[0], ng[None]
    bf, f32 = jnp.bfloat16, jnp.float32
    rows, chans = og.shape
    lane_rows, width = ei.shape
    n_x = n_tp // CORES
    sems = 2 * n_ep + 2
    big = (og, ig, va, taps, mw, ei, ng, gw, uw, dw, sg, su, sd)
    out = jax.ShapeDtypeStruct((rows, chans), bf)
    vmem = pl.BlockSpec(memory_space=pltpu.VMEM)
    dma = pltpu.SemaphoreType.DMA
    return pl.pallas_call(
        functools.partial(kernel, n_ep, n_tp),
        out_shape=(out, out),
        in_specs=[vmem, vmem] + [pl.BlockSpec(memory_space=pl.ANY)] * len(big),
        out_specs=(vmem, vmem),
        scratch_shapes=[pltpu.VMEM(a.shape, a.dtype) for a in big]
        + [
            pltpu.VMEM((n_ep, n_tp, lane_rows, width), bf),
            pltpu.VMEM((n_ep, n_tp, rows, gw.shape[-1]), bf),
            pltpu.VMEM((n_tp, rows, sg.shape[-1]), bf),
            pltpu.VMEM((n_tp, rows, chans), bf),
            pltpu.VMEM((rows, chans), bf),
            pltpu.VMEM((16, chans), bf),
            pltpu.VMEM((n_ep, rows, chans), bf),
            pltpu.VMEM((n_ep + 1, rows, chans), bf),
            pltpu.VMEM((n_ep, -(-n_ep // 8) * 8, -(-rows // 128) * 128), f32),
            dma((len(big),)),
            dma((2, n_ep)),
            dma((n_ep,)),
            dma((sems, max(1, n_x - 1))),
            dma((sems, max(1, n_x - 1))),
            dma((sems, n_x)),
            dma((sems, n_x)),
            dma((n_ep, CHUNKS)),
            dma((n_ep + 1, CHUNKS)),
            dma((n_ep,)),
            dma((n_ep,)),
            dma((2,)),
        ],
        compiler_params=pltpu.CompilerParams(
            collective_id=0, has_side_effects=True, vmem_limit_bytes=60 * 1024 * 1024
        ),
    )(ids.T, rw.T, *big)


def local(*args):
    n_ep, n_tp = lax.axis_size("ep"), lax.axis_size("tp")
    chans, lane_rows = args[0].shape[1], args[5].shape[0]
    aligned = (
        n_tp % CORES == 0
        and lane_rows % 16 == 0
        and lane_rows * n_tp == args[0].shape[0]
        and chans % TILE == 0
        and args[0].shape[0] % (16 * CHUNKS) == 0
        and args[9].shape[2] % 128 == 0
        and args[12].shape[1] % 128 == 0
    )
    return joined(n_ep, n_tp, *args) if aligned else plain(*args)


def solution(mesh):
    placed = (
        P(("grp", "ep"), "tp"),
        P(("grp", "ep"), "tp"),
        P(("grp", "ep"), "tp"),
        P(None, "tp"),
        P(None, "tp"),
        P(("grp", "ep", "tp"), None),
        P(),
        P(("grp", "ep"), None),
        P(("grp", "ep"), None),
        P("ep", None, "tp"),
        P("ep", None, "tp"),
        P("ep", None, "tp"),
        P(None, "tp"),
        P(None, "tp"),
        P(None, "tp"),
    )
    return jax.shard_map(
        local,
        mesh=mesh,
        in_specs=placed,
        out_specs=(P(("grp", "ep"), "tp"), P(("grp", "ep"), "tp")),
        check_vma=False,
    )
```

```python
import functools

import jax
import jax.numpy as jnp
from jax import lax
from jax.experimental import pallas as pl
from jax.experimental.pallas import tpu as pltpu
from jax.sharding import PartitionSpec as P

MESH = pl.DeviceIdType.MESH
CORES = 2
TILE = 256
PIECE = 16
CHUNKS = 4

norm_floor = 0.5


def shifted(value, axis, steps):
    count = lax.axis_size(axis)
    leading, last = (max(0, -steps), min(count, count - steps))
    return lax.ppermute(value, axis, [(source, source + steps) for source in range(leading, last)])


def layer_norm(tokens, norm_gain):
    widened = tokens.astype(jnp.float32)
    centred = widened - jnp.mean(widened, axis=-1, keepdims=True)
    spread = jnp.mean(centred * centred, axis=-1, keepdims=True)
    return (centred * lax.rsqrt(spread + norm_floor) * norm_gain).astype(jnp.bfloat16)


def expert_hidden(inputs, gate_part, up_part):
    gate_value = jnp.dot(inputs, gate_part, preferred_element_type=jnp.float32)
    up_value = jnp.dot(inputs, up_part, preferred_element_type=jnp.float32)
    return (jax.nn.silu(gate_value) * up_value).astype(jnp.bfloat16)


def slot_ranks(route_ids, experts, lanes):
    tok_count, top_count = route_ids.shape
    grouped = route_ids.reshape(lanes, tok_count // lanes * top_count)
    onehot = (grouped[:, :, None] == jnp.arange(experts, dtype=jnp.int32)[None, None, :]).astype(
        jnp.int32
    )
    before = jnp.cumsum(onehot, axis=1) - onehot
    return jnp.sum(before * onehot, axis=2).reshape(tok_count, top_count)


def plain(
    out_gate,
    in_gate,
    values,
    conv_taps,
    mixer_weight,
    expert_input,
    norm_gain,
    route_ids,
    route_weights,
    gate_weight,
    up_weight,
    down_weight,
    shared_gate,
    shared_up,
    shared_down,
):
    experts = lax.axis_size("ep")
    lanes = lax.axis_size("tp")
    lane_rows = expert_input.shape[0]
    width = expert_input.shape[1]
    tok_count, top_count = route_ids.shape
    capacity = (2 * lane_rows * top_count + experts - 1) // experts
    gated_values = (in_gate.astype(jnp.float32) * values.astype(jnp.float32)).astype(jnp.bfloat16)
    previous = shifted(gated_values[-2:], "ep", 1)
    extended = jnp.concatenate([previous, gated_values], axis=0).astype(jnp.float32)
    conv_state = (
        conv_taps[0] * extended[:-2] + conv_taps[1] * extended[1:-1] + conv_taps[2] * extended[2:]
    )
    mixed_rows = (out_gate.astype(jnp.float32) * conv_state).astype(jnp.bfloat16)
    normed_own = layer_norm(expert_input, norm_gain)
    mixed_whole, normed_rows = (
        lax.all_gather(mixed_rows, "tp", axis=1, tiled=True),
        lax.all_gather(normed_own, "tp", axis=0, tiled=True),
    )
    mixer_output = jnp.dot(mixed_whole, mixer_weight, preferred_element_type=jnp.float32).astype(
        jnp.bfloat16
    )
    shared_part = expert_hidden(normed_rows, shared_gate, shared_up)
    slot_index = slot_ranks(route_ids, experts, lanes)
    lane_of_row = (jnp.arange(tok_count, dtype=jnp.int32) // lane_rows)[:, None]
    positions = (route_ids * lanes + lane_of_row) * capacity + slot_index
    lane_index = lax.axis_index("tp")
    lane_ids = lax.dynamic_slice_in_dim(route_ids, lane_index * lane_rows, lane_rows, 0)
    lane_slots = lax.dynamic_slice_in_dim(slot_index, lane_index * lane_rows, lane_rows, 0)
    lane_places = lane_ids * capacity + lane_slots
    local_rows = jnp.broadcast_to(jnp.arange(lane_rows, dtype=jnp.int32)[:, None], lane_ids.shape)
    owners = jnp.full((experts * capacity,), lane_rows, jnp.int32)
    owners = owners.at[lane_places.reshape(-1)].set(local_rows.reshape(-1))
    outgoing = jnp.take(normed_own, owners, axis=0, mode="fill", fill_value=0)
    arrived = lax.all_to_all(
        outgoing.reshape(experts, capacity, width), "ep", split_axis=0, concat_axis=0, tiled=True
    )
    segment = lax.all_gather(arrived[None], "tp", axis=0, tiled=True)
    hidden_rows = expert_hidden(segment.reshape(-1, width), gate_weight[0], up_weight[0])
    spread_hidden = hidden_rows.reshape(segment.shape[:-1] + (hidden_rows.shape[-1],))
    routed_hidden = jnp.swapaxes(spread_hidden, 0, 1).reshape(-1, spread_hidden.shape[-1])
    routed_whole, shared_whole = (
        lax.all_gather(routed_hidden, "tp", axis=1, tiled=True),
        lax.all_gather(shared_part, "tp", axis=1, tiled=True),
    )
    routed_result = jnp.dot(
        routed_whole, down_weight[0], preferred_element_type=jnp.float32
    ).astype(jnp.bfloat16)
    out_cols = routed_result.shape[-1]
    returned = lax.all_to_all(
        routed_result.reshape(experts, lanes * capacity, out_cols),
        "ep",
        split_axis=0,
        concat_axis=0,
        tiled=True,
    )
    shared_result = jnp.dot(shared_whole, shared_down, preferred_element_type=jnp.float32)
    picked = jnp.take(
        returned.reshape(experts * lanes * capacity, out_cols), positions.reshape(-1), axis=0
    )
    picked = picked.astype(jnp.float32).reshape(tok_count, top_count, out_cols)
    expert_output = (shared_result + jnp.sum(route_weights[:, :, None] * picked, axis=1)).astype(
        jnp.bfloat16
    )
    return (mixer_output, expert_output)


def silu_product(gate_value, up_value):
    return (gate_value * (1.0 / (1.0 + jnp.exp(-gate_value))) * up_value).astype(jnp.bfloat16)


def dot32(left, right):
    return jnp.dot(left, right, preferred_element_type=jnp.float32)


def kernel(
    n_ep,
    n_tp,
    ids,
    rw,
    og_h,
    ig_h,
    va_h,
    taps_h,
    mw_h,
    ei_h,
    ng_h,
    gw_h,
    uw_h,
    dw_h,
    sg_h,
    su_h,
    sd_h,
    mix_out,
    exp_out,
    og,
    ig,
    va,
    taps,
    mw,
    ei,
    ng,
    gw,
    uw,
    dw,
    sg,
    su,
    sd,
    tok,
    hid,
    shd,
    mixed,
    gated,
    halo,
    res,
    pin,
    wts,
    ld,
    z_send,
    z_recv,
    x_send,
    x_recv,
    p_send,
    p_recv,
    r_send,
    r_recv,
    w_send,
    w_recv,
    h_sem,
):
    e = lax.axis_index("ep")
    t = lax.axis_index("tp")
    n_x = n_tp // CORES
    partner = t + 1 - 2 * (t % CORES)
    lane_rows, width = ei.shape
    rows, chans = og.shape

    loads = {}
    for number, (name, src, dst) in enumerate(
        (
            ("ei", ei_h, ei),
            ("ng", ng_h, ng),
            ("ig", ig_h, ig),
            ("va", va_h, va),
            ("og", og_h, og),
            ("taps", taps_h, taps),
            ("gw", gw_h, gw),
            ("uw", uw_h, uw),
            ("sg", sg_h, sg),
            ("su", su_h, su),
            ("dw", dw_h, dw),
            ("sd", sd_h, sd),
            ("mw", mw_h, mw),
        )
    ):
        loads[name] = pltpu.make_async_copy(src, dst, ld.at[number])
        loads[name].start()

    barrier = pltpu.get_barrier_semaphore()
    greeted = [{"ep": (e + d) % n_ep, "tp": t} for d in range(1, n_ep)]
    greeted += [{"ep": e, "tp": (t + CORES * d) % n_tp} for d in range(1, n_x)]
    greeted += [{"ep": e, "tp": partner}]
    for peer in greeted:
        pl.semaphore_signal(barrier, inc=1, device_id=peer, device_id_type=MESH)

    def remote(src, dst, send, recv, ep, tp):
        return pltpu.make_async_remote_copy(
            src_ref=src,
            dst_ref=dst,
            send_sem=send,
            recv_sem=recv,
            device_id={"ep": ep, "tp": tp},
            device_id_type=MESH,
        )

    def cross(slot, g, d, lane):
        return remote(
            slot(lane), slot(lane), x_send.at[g, d - 1], x_recv.at[g, d - 1],
            e, (t + CORES * d) % n_tp,
        )

    def across(slot, g, d, lane):
        return remote(slot(lane), slot(lane), p_send.at[g, d], p_recv.at[g, d], e, partner)

    def from_x(d):
        return (t + n_tp - CORES * d) % n_tp

    def from_partner(d):
        return (partner + n_tp - CORES * d) % n_tp

    def gather_start(slot, g):
        for d in range(1, n_x):
            cross(slot, g, d, t).start()
        across(slot, g, 0, t).start()

    def gather_forward(slot, g):
        for d in range(1, n_x):
            cross(slot, g, d, from_x(d)).wait_recv()
            across(slot, g, d, from_x(d)).start()

    def gather_finish(slot, g):
        for d in range(n_x):
            across(slot, g, d, from_partner(d)).wait_recv()

    def gather_drain(slot, g):
        for d in range(1, n_x):
            cross(slot, g, d, t).wait_send()
            across(slot, g, d, from_x(d)).wait_send()
        across(slot, g, 0, t).wait_send()

    pieces = lane_rows // PIECE
    first_hidden = n_ep * pieces
    shared_g = first_hidden + n_ep
    mixed_g = shared_g + 1

    def tok_slot(j, q):
        return lambda lane: tok.at[j, lane, q]

    def hid_slot(j):
        return lambda lane: hid.at[j, lane]

    def shd_slot(lane):
        return shd.at[lane]

    def mixed_slot(lane):
        return mixed.at[lane]

    nearest = jnp.minimum(e, n_ep - 1 - e)
    left_short = e <= n_ep - 1 - e

    def block_at(k):
        near = jnp.where(k % 2 == 1, e - (k + 1) // 2, e + k // 2)
        far = jnp.where(left_short, k, n_ep - 1 - k)
        return jnp.where(k <= 2 * nearest, near, far)

    def at_end(j):
        return (j == 0) | (j == n_ep - 1)

    def crosses(j):
        return (j == e) | ~at_end(j)

    def z_copy(side, d, j, q):
        block = tok.at[j, from_x(d), q]
        return remote(block, block, z_send.at[side, d, j, q], z_recv.at[d, j, q],
                      jnp.clip(e + 1 - 2 * side, 0, n_ep - 1), t)

    def goes_right(j):
        return (j <= e) & (e < n_ep - 1)

    def goes_left(j):
        return (j >= e) & (e > 0)

    def z_onward(d, j, q):
        @pl.when(goes_right(j))
        def _():
            z_copy(0, d, j, q).start()

        @pl.when(goes_left(j))
        def _():
            z_copy(1, d, j, q).start()

    def spread(k, q):
        j = block_at(k)
        g = j * pieces + q

        @pl.when(k > 0)
        def _():
            z_copy(0, 0, j, q).wait_recv()

        z_onward(0, j, q)

        @pl.when(crosses(j))
        def _():
            for d in range(1, n_x):
                cross(tok_slot(j, q), g, d, t).start()

        across(tok_slot(j, q), g, 0, t).start()

    def forward(k, q):
        j = block_at(k)
        g = j * pieces + q
        for d in range(1, n_x):

            @pl.when(crosses(j))
            def _():
                cross(tok_slot(j, q), g, d, from_x(d)).wait_recv()

            @pl.when(~crosses(j))
            def _():
                z_copy(0, d, j, q).wait_recv()

            @pl.when(at_end(j))
            def _():
                z_onward(d, j, q)

            across(tok_slot(j, q), g, d, from_x(d)).start()

    piece = rows // CHUNKS

    def hop(j, c):
        at = pl.ds(pl.multiple_of(c * piece, 16), piece)
        after = jnp.clip(jnp.where(j > e, e + 1, e - 1), 0, n_ep - 1)
        slot = jnp.where((j < e) & (after == j), n_ep, j)
        return remote(res.at[j, at], pin.at[slot, at], r_send.at[j, c], r_recv.at[slot, c], after, t)

    def hop_arrives(slot, c):
        at = pl.ds(pl.multiple_of(c * piece, 16), piece)
        remote(res.at[0, at], pin.at[slot, at], r_send.at[0, c], r_recv.at[slot, c],
               jnp.clip(e + 1, 0, n_ep - 1), t).wait_recv()

    inner = (e > 0) & (e < n_ep - 1)

    def weights_to(d):
        return remote(wts.at[e], wts.at[e], w_send.at[d - 1], w_recv.at[e], (e + d) % n_ep, t)

    def weight_column(j):
        held = wts[j]
        mine = jnp.where(lax.broadcasted_iota(jnp.int32, held.shape, 0) == e, held, 0.0)
        line = jnp.sum(mine, axis=0, keepdims=True)
        shape = (rows, held.shape[1])
        same = lax.broadcasted_iota(jnp.int32, shape, 0) == lax.broadcasted_iota(jnp.int32, shape, 1)
        return jnp.sum(jnp.where(same, line, 0.0), axis=1, keepdims=True)

    loads["ei"].wait()
    loads["ng"].wait()

    def norm_rows(r, _):
        at = pl.ds(pl.multiple_of(r * PIECE, PIECE), PIECE)
        widened = ei[at, :].astype(jnp.float32)
        centred = widened - jnp.mean(widened, axis=-1, keepdims=True)
        spread_of = jnp.mean(centred * centred, axis=-1, keepdims=True)
        normed = centred * lax.rsqrt(spread_of + norm_floor) * ng[...]
        tok[e, t, r] = normed.astype(jnp.bfloat16)
        return 0

    lax.fori_loop(0, pieces, norm_rows, 0)
    pl.semaphore_wait(barrier, len(greeted))
    for q in range(pieces):
        spread(0, q)

    place = lax.broadcasted_iota(jnp.int32, (wts.shape[1], rows), 0)
    dense = jnp.zeros(place.shape, jnp.float32)
    for k in range(ids.shape[0]):
        dense += jnp.where(ids[k : k + 1, :] == place, rw[k : k + 1, :], 0.0)
    wts[e] = jnp.zeros(wts.shape[1:], jnp.float32)
    wts[e, :, 0:rows] = dense
    for d in range(1, n_ep):
        weights_to(d).start()

    loads["ig"].wait()
    loads["va"].wait()

    def gate_cols(c, _):
        at = pl.ds(pl.multiple_of(c * 128, 128), 128)
        gated[:, at] = (ig[:, at].astype(jnp.float32) * va[:, at].astype(jnp.float32)).astype(
            jnp.bfloat16
        )
        return 0

    lax.fori_loop(0, chans // 128, gate_cols, 0)

    def halo_copy():
        return remote(gated.at[pl.ds(rows - 16, 16)], halo, h_sem.at[0], h_sem.at[1],
                      jnp.minimum(e + 1, n_ep - 1), t)

    @pl.when(e < n_ep - 1)
    def _():
        halo_copy().start()

    loads["og"].wait()
    loads["taps"].wait()

    @pl.when(e == 0)
    def _():
        halo[...] = jnp.zeros_like(halo)

    @pl.when(e > 0)
    def _():
        halo_copy().wait_recv()

    def mix_cols(c, _):
        at = pl.ds(pl.multiple_of(c * 128, 128), 128)
        now = gated[:, at].astype(jnp.float32)
        before = halo[:, at].astype(jnp.float32)
        place = lax.broadcasted_iota(jnp.int32, now.shape, 0)
        one = jnp.where(place == 0, before[15:16], pltpu.roll(now, 1, 0))
        two = jnp.where(
            place == 0, before[14:15], jnp.where(place == 1, before[15:16], pltpu.roll(now, 2, 0))
        )
        state = taps[0:1, at] * two + taps[1:2, at] * one + taps[2:3, at] * now
        mixed[t, :, at] = (og[:, at].astype(jnp.float32) * state).astype(jnp.bfloat16)
        return 0

    lax.fori_loop(0, chans // 128, mix_cols, 0)
    for name in ("gw", "uw", "sg", "su"):
        loads[name].wait()

    def step(s, _):
        for q in range(pieces):

            @pl.when(s + 1 < n_ep)
            def _():
                spread(s + 1, q)

            @pl.when(s < n_ep)
            def _():
                forward(s, q)

        @pl.when(s >= 1)
        def _():
            j = block_at(s - 1)
            gather_forward(hid_slot(j), first_hidden + j)
            gather_finish(hid_slot(j), first_hidden + j)
            part = hid.shape[-1]

            @pl.when(j != e)
            def _():
                remote(wts.at[e], wts.at[j], w_send.at[0], w_recv.at[j], j, t).wait_recv()

            weight = weight_column(j)
            for c in range(chans // TILE):
                at = slice(c * TILE, (c + 1) * TILE)
                total = dot32(hid[j, 0], dw[0:part, at])
                for lane in range(1, n_tp):
                    total += dot32(hid[j, lane], dw[lane * part : (lane + 1) * part, at])
                res[j, :, at] = (weight * total).astype(jnp.bfloat16)

            @pl.when((j != e) & ~inner)
            def _():
                for c in range(CHUNKS):
                    hop(j, c).start()

        @pl.when(s < n_ep)
        def _():
            j = block_at(s)
            for q in range(pieces):
                gather_finish(tok_slot(j, q), j * pieces + q)
            block = tok[j].reshape(rows, width)
            hid[j, t] = silu_product(dot32(block, gw[...]), dot32(block, uw[...]))
            gather_start(hid_slot(j), first_hidden + j)

        @pl.when(s == 0)
        def _():
            block = tok[e].reshape(rows, width)
            shd[t] = silu_product(dot32(block, sg[...]), dot32(block, su[...]))
            gather_start(shd_slot, shared_g)
            loads["dw"].wait()

        @pl.when(s == n_ep - 1)
        def _():
            gather_start(mixed_slot, mixed_g)

        return 0

    lax.fori_loop(0, n_ep + 1, step, 0)

    gather_forward(shd_slot, shared_g)

    for phase in range(2):
        right = left_short if phase == 0 else ~left_short

        def relay(d, _):
            j = jnp.where(right, e + d, e - d)

            @pl.when(inner & (j >= 0) & (j < n_ep))
            def _():
                def relay_piece(c, _):
                    at = pl.ds(pl.multiple_of(c * piece, 16), piece)
                    hop_arrives(j, c)
                    total = res[j, at, :].astype(jnp.float32) + pin[j, at, :].astype(jnp.float32)
                    res[j, at, :] = total.astype(jnp.bfloat16)
                    hop(j, c).start()
                    return 0

                lax.fori_loop(0, CHUNKS, relay_piece, 0)

            return 0

        lax.fori_loop(1, n_ep, relay, 0)

    gather_forward(mixed_slot, mixed_g)
    gather_finish(shd_slot, shared_g)
    loads["sd"].wait()
    loads["mw"].wait()
    gather_finish(mixed_slot, mixed_g)

    def mixer_cols(c, _):
        at = pl.ds(pl.multiple_of(c * TILE, TILE), TILE)
        total = dot32(mixed[0], mw[0:chans, at])
        for lane in range(1, n_tp):
            total += dot32(mixed[lane], mw[lane * chans : (lane + 1) * chans, at])
        mix_out[:, at] = total.astype(jnp.bfloat16)
        return 0

    lax.fori_loop(0, chans // TILE, mixer_cols, 0)

    for here, slot in ((e > 0, e), (e < n_ep - 1, n_ep)):

        @pl.when(here)
        def _():
            for c in range(CHUNKS):
                hop_arrives(slot, c)

        @pl.when(~here)
        def _():
            pin[slot] = jnp.zeros(pin.shape[1:], pin.dtype)

    def combine_cols(c, _):
        at = pl.ds(pl.multiple_of(c * TILE, TILE), TILE)
        part = shd.shape[-1]
        total = dot32(shd[0], sd[0:part, at])
        for lane in range(1, n_tp):
            total += dot32(shd[lane], sd[lane * part : (lane + 1) * part, at])
        for found in (res[e, :, at], pin[e, :, at], pin[n_ep, :, at]):
            total += found.astype(jnp.float32)
        exp_out[:, at] = total.astype(jnp.bfloat16)
        return 0

    lax.fori_loop(0, chans // TILE, combine_cols, 0)

    @pl.when(e < n_ep - 1)
    def _():
        halo_copy().wait_send()

    def drain(j, _):
        def drain_z(d, q):
            @pl.when(goes_right(j))
            def _():
                z_copy(0, d, j, q).wait_send()

            @pl.when(goes_left(j))
            def _():
                z_copy(1, d, j, q).wait_send()

        for q in range(pieces):
            g = j * pieces + q
            drain_z(0, q)
            across(tok_slot(j, q), g, 0, t).wait_send()
            for d in range(1, n_x):

                @pl.when(crosses(j))
                def _():
                    cross(tok_slot(j, q), g, d, t).wait_send()

                @pl.when(at_end(j))
                def _():
                    drain_z(d, q)

                across(tok_slot(j, q), g, d, from_x(d)).wait_send()

        gather_drain(hid_slot(j), first_hidden + j)

        @pl.when(j != e)
        def _():
            for c in range(CHUNKS):
                hop(j, c).wait_send()

        return 0

    lax.fori_loop(0, n_ep, drain, 0)
    for d in range(1, n_ep):
        weights_to(d).wait_send()
    gather_drain(shd_slot, shared_g)
    gather_drain(mixed_slot, mixed_g)


def joined(n_ep, n_tp, *args):
    (og, ig, va, taps, mw, ei, ng, ids, rw, gw, uw, dw, sg, su, sd) = args
    gw, uw, dw, ng = gw[0], uw[0], dw[0], ng[None]
    bf, f32 = jnp.bfloat16, jnp.float32
    rows, chans = og.shape
    lane_rows, width = ei.shape
    n_x = n_tp // CORES
    pieces = lane_rows // PIECE
    sems = n_ep * pieces + n_ep + 2
    big = (og, ig, va, taps, mw, ei, ng, gw, uw, dw, sg, su, sd)
    out = jax.ShapeDtypeStruct((rows, chans), bf)
    vmem = pl.BlockSpec(memory_space=pltpu.VMEM)
    dma = pltpu.SemaphoreType.DMA
    return pl.pallas_call(
        functools.partial(kernel, n_ep, n_tp),
        out_shape=(out, out),
        in_specs=[vmem, vmem] + [pl.BlockSpec(memory_space=pl.ANY)] * len(big),
        out_specs=(vmem, vmem),
        scratch_shapes=[pltpu.VMEM(a.shape, a.dtype) for a in big]
        + [
            pltpu.VMEM((n_ep, n_tp, pieces, PIECE, width), bf),
            pltpu.VMEM((n_ep, n_tp, rows, gw.shape[-1]), bf),
            pltpu.VMEM((n_tp, rows, sg.shape[-1]), bf),
            pltpu.VMEM((n_tp, rows, chans), bf),
            pltpu.VMEM((rows, chans), bf),
            pltpu.VMEM((16, chans), bf),
            pltpu.VMEM((n_ep, rows, chans), bf),
            pltpu.VMEM((n_ep + 1, rows, chans), bf),
            pltpu.VMEM((n_ep, -(-n_ep // 8) * 8, -(-rows // 128) * 128), f32),
            dma((len(big),)),
            dma((2, n_x, n_ep, pieces)),
            dma((n_x, n_ep, pieces)),
            dma((sems, max(1, n_x - 1))),
            dma((sems, max(1, n_x - 1))),
            dma((sems, n_x)),
            dma((sems, n_x)),
            dma((n_ep, CHUNKS)),
            dma((n_ep + 1, CHUNKS)),
            dma((n_ep,)),
            dma((n_ep,)),
            dma((2,)),
        ],
        compiler_params=pltpu.CompilerParams(
            collective_id=0, has_side_effects=True, vmem_limit_bytes=60 * 1024 * 1024
        ),
    )(ids.T, rw.T, *big)


def local(*args):
    n_ep, n_tp = lax.axis_size("ep"), lax.axis_size("tp")
    chans, lane_rows = args[0].shape[1], args[5].shape[0]
    aligned = (
        n_tp % CORES == 0
        and lane_rows % PIECE == 0
        and lane_rows * n_tp == args[0].shape[0]
        and chans % TILE == 0
        and args[0].shape[0] % (16 * CHUNKS) == 0
        and args[9].shape[2] % 128 == 0
        and args[12].shape[1] % 128 == 0
    )
    return joined(n_ep, n_tp, *args) if aligned else plain(*args)


def solution(mesh):
    placed = (
        P(("grp", "ep"), "tp"),
        P(("grp", "ep"), "tp"),
        P(("grp", "ep"), "tp"),
        P(None, "tp"),
        P(None, "tp"),
        P(("grp", "ep", "tp"), None),
        P(),
        P(("grp", "ep"), None),
        P(("grp", "ep"), None),
        P("ep", None, "tp"),
        P("ep", None, "tp"),
        P("ep", None, "tp"),
        P(None, "tp"),
        P(None, "tp"),
        P(None, "tp"),
    )
    return jax.shard_map(
        local,
        mesh=mesh,
        in_specs=placed,
        out_specs=(P(("grp", "ep"), "tp"), P(("grp", "ep"), "tp")),
        check_vma=False,
    )
```

```python
import functools

import jax
import jax.numpy as jnp
from jax import lax
from jax.experimental import pallas as pl
from jax.experimental.pallas import tpu as pltpu
from jax.sharding import PartitionSpec as P

MESH = pl.DeviceIdType.MESH
CORES = 2
TILE = 256
PIECE = 16
CHUNKS = 4

norm_floor = 0.5


def shifted(value, axis, steps):
    count = lax.axis_size(axis)
    leading, last = (max(0, -steps), min(count, count - steps))
    return lax.ppermute(value, axis, [(source, source + steps) for source in range(leading, last)])


def layer_norm(tokens, norm_gain):
    widened = tokens.astype(jnp.float32)
    centred = widened - jnp.mean(widened, axis=-1, keepdims=True)
    spread = jnp.mean(centred * centred, axis=-1, keepdims=True)
    return (centred * lax.rsqrt(spread + norm_floor) * norm_gain).astype(jnp.bfloat16)


def expert_hidden(inputs, gate_part, up_part):
    gate_value = jnp.dot(inputs, gate_part, preferred_element_type=jnp.float32)
    up_value = jnp.dot(inputs, up_part, preferred_element_type=jnp.float32)
    return (jax.nn.silu(gate_value) * up_value).astype(jnp.bfloat16)


def slot_ranks(route_ids, experts, lanes):
    tok_count, top_count = route_ids.shape
    grouped = route_ids.reshape(lanes, tok_count // lanes * top_count)
    onehot = (grouped[:, :, None] == jnp.arange(experts, dtype=jnp.int32)[None, None, :]).astype(
        jnp.int32
    )
    before = jnp.cumsum(onehot, axis=1) - onehot
    return jnp.sum(before * onehot, axis=2).reshape(tok_count, top_count)


def plain(
    out_gate,
    in_gate,
    values,
    conv_taps,
    mixer_weight,
    expert_input,
    norm_gain,
    route_ids,
    route_weights,
    gate_weight,
    up_weight,
    down_weight,
    shared_gate,
    shared_up,
    shared_down,
):
    experts = lax.axis_size("ep")
    lanes = lax.axis_size("tp")
    lane_rows = expert_input.shape[0]
    width = expert_input.shape[1]
    tok_count, top_count = route_ids.shape
    capacity = (2 * lane_rows * top_count + experts - 1) // experts
    gated_values = (in_gate.astype(jnp.float32) * values.astype(jnp.float32)).astype(jnp.bfloat16)
    previous = shifted(gated_values[-2:], "ep", 1)
    extended = jnp.concatenate([previous, gated_values], axis=0).astype(jnp.float32)
    conv_state = (
        conv_taps[0] * extended[:-2] + conv_taps[1] * extended[1:-1] + conv_taps[2] * extended[2:]
    )
    mixed_rows = (out_gate.astype(jnp.float32) * conv_state).astype(jnp.bfloat16)
    normed_own = layer_norm(expert_input, norm_gain)
    mixed_whole, normed_rows = (
        lax.all_gather(mixed_rows, "tp", axis=1, tiled=True),
        lax.all_gather(normed_own, "tp", axis=0, tiled=True),
    )
    mixer_output = jnp.dot(mixed_whole, mixer_weight, preferred_element_type=jnp.float32).astype(
        jnp.bfloat16
    )
    shared_part = expert_hidden(normed_rows, shared_gate, shared_up)
    slot_index = slot_ranks(route_ids, experts, lanes)
    lane_of_row = (jnp.arange(tok_count, dtype=jnp.int32) // lane_rows)[:, None]
    positions = (route_ids * lanes + lane_of_row) * capacity + slot_index
    lane_index = lax.axis_index("tp")
    lane_ids = lax.dynamic_slice_in_dim(route_ids, lane_index * lane_rows, lane_rows, 0)
    lane_slots = lax.dynamic_slice_in_dim(slot_index, lane_index * lane_rows, lane_rows, 0)
    lane_places = lane_ids * capacity + lane_slots
    local_rows = jnp.broadcast_to(jnp.arange(lane_rows, dtype=jnp.int32)[:, None], lane_ids.shape)
    owners = jnp.full((experts * capacity,), lane_rows, jnp.int32)
    owners = owners.at[lane_places.reshape(-1)].set(local_rows.reshape(-1))
    outgoing = jnp.take(normed_own, owners, axis=0, mode="fill", fill_value=0)
    arrived = lax.all_to_all(
        outgoing.reshape(experts, capacity, width), "ep", split_axis=0, concat_axis=0, tiled=True
    )
    segment = lax.all_gather(arrived[None], "tp", axis=0, tiled=True)
    hidden_rows = expert_hidden(segment.reshape(-1, width), gate_weight[0], up_weight[0])
    spread_hidden = hidden_rows.reshape(segment.shape[:-1] + (hidden_rows.shape[-1],))
    routed_hidden = jnp.swapaxes(spread_hidden, 0, 1).reshape(-1, spread_hidden.shape[-1])
    routed_whole, shared_whole = (
        lax.all_gather(routed_hidden, "tp", axis=1, tiled=True),
        lax.all_gather(shared_part, "tp", axis=1, tiled=True),
    )
    routed_result = jnp.dot(
        routed_whole, down_weight[0], preferred_element_type=jnp.float32
    ).astype(jnp.bfloat16)
    out_cols = routed_result.shape[-1]
    returned = lax.all_to_all(
        routed_result.reshape(experts, lanes * capacity, out_cols),
        "ep",
        split_axis=0,
        concat_axis=0,
        tiled=True,
    )
    shared_result = jnp.dot(shared_whole, shared_down, preferred_element_type=jnp.float32)
    picked = jnp.take(
        returned.reshape(experts * lanes * capacity, out_cols), positions.reshape(-1), axis=0
    )
    picked = picked.astype(jnp.float32).reshape(tok_count, top_count, out_cols)
    expert_output = (shared_result + jnp.sum(route_weights[:, :, None] * picked, axis=1)).astype(
        jnp.bfloat16
    )
    return (mixer_output, expert_output)


def silu_product(gate_value, up_value):
    return (gate_value * (1.0 / (1.0 + jnp.exp(-gate_value))) * up_value).astype(jnp.bfloat16)


def dot32(left, right):
    return jnp.dot(left, right, preferred_element_type=jnp.float32)


def kernel(
    n_ep,
    n_tp,
    ids,
    rw,
    og_h,
    ig_h,
    va_h,
    taps_h,
    mw_h,
    ei_h,
    ng_h,
    gw_h,
    uw_h,
    dw_h,
    sg_h,
    su_h,
    sd_h,
    mix_out,
    exp_out,
    og,
    ig,
    va,
    taps,
    mw,
    ei,
    ng,
    gw,
    uw,
    dw,
    sg,
    su,
    sd,
    tok,
    hid,
    shd,
    mixed,
    gated,
    halo,
    res,
    pin,
    wts,
    ld,
    z_send,
    z_recv,
    x_send,
    x_recv,
    p_send,
    p_recv,
    r_send,
    r_recv,
    w_send,
    w_recv,
    h_sem,
):
    e = lax.axis_index("ep")
    t = lax.axis_index("tp")
    n_x = n_tp // CORES
    partner = t + 1 - 2 * (t % CORES)
    lane_rows, width = ei.shape
    rows, chans = og.shape

    loads = {}
    for number, (name, src, dst) in enumerate(
        (
            ("ei", ei_h, ei),
            ("ng", ng_h, ng),
            ("ig", ig_h, ig),
            ("va", va_h, va),
            ("og", og_h, og),
            ("taps", taps_h, taps),
            ("gw", gw_h, gw),
            ("uw", uw_h, uw),
            ("sg", sg_h, sg),
            ("su", su_h, su),
            ("dw", dw_h, dw),
            ("sd", sd_h, sd),
            ("mw", mw_h, mw),
        )
    ):
        loads[name] = pltpu.make_async_copy(src, dst, ld.at[number])
        loads[name].start()

    barrier = pltpu.get_barrier_semaphore()
    greeted = [{"ep": (e + d) % n_ep, "tp": t} for d in range(1, n_ep)]
    greeted += [{"ep": e, "tp": (t + CORES * d) % n_tp} for d in range(1, n_x)]
    greeted += [{"ep": e, "tp": partner}]
    for peer in greeted:
        pl.semaphore_signal(barrier, inc=1, device_id=peer, device_id_type=MESH)

    def remote(src, dst, send, recv, ep, tp):
        return pltpu.make_async_remote_copy(
            src_ref=src,
            dst_ref=dst,
            send_sem=send,
            recv_sem=recv,
            device_id={"ep": ep, "tp": tp},
            device_id_type=MESH,
        )

    def cross(slot, g, d, lane):
        return remote(
            slot(lane), slot(lane), x_send.at[g, d - 1], x_recv.at[g, d - 1],
            e, (t + CORES * d) % n_tp,
        )

    def across(slot, g, d, lane):
        return remote(slot(lane), slot(lane), p_send.at[g, d], p_recv.at[g, d], e, partner)

    def from_x(d):
        return (t + n_tp - CORES * d) % n_tp

    def from_partner(d):
        return (partner + n_tp - CORES * d) % n_tp

    def gather_start(slot, g):
        for d in range(1, n_x):
            cross(slot, g, d, t).start()
        across(slot, g, 0, t).start()

    def gather_forward(slot, g):
        for d in range(1, n_x):
            cross(slot, g, d, from_x(d)).wait_recv()
            across(slot, g, d, from_x(d)).start()

    def gather_finish(slot, g):
        for d in range(n_x):
            across(slot, g, d, from_partner(d)).wait_recv()

    def gather_drain(slot, g):
        for d in range(1, n_x):
            cross(slot, g, d, t).wait_send()
            across(slot, g, d, from_x(d)).wait_send()
        across(slot, g, 0, t).wait_send()

    pieces = lane_rows // PIECE
    first_hidden = n_ep * pieces
    shared_g = first_hidden + n_ep
    mixed_g = shared_g + 1

    def tok_slot(j, q):
        return lambda lane: tok.at[j, lane, q]

    def hid_slot(j):
        return lambda lane: hid.at[j, lane]

    def shd_slot(lane):
        return shd.at[lane]

    def mixed_slot(lane):
        return mixed.at[lane]

    nearest = jnp.minimum(e, n_ep - 1 - e)
    left_short = e <= n_ep - 1 - e

    def block_at(k):
        near = jnp.where(k % 2 == 1, e - (k + 1) // 2, e + k // 2)
        far = jnp.where(left_short, k, n_ep - 1 - k)
        return jnp.where(k <= 2 * nearest, near, far)

    def at_end(j):
        return (j == 0) | (j == n_ep - 1)

    def crosses(j):
        return (j == e) | ~at_end(j)

    def z_copy(side, d, j, q):
        block = tok.at[j, from_x(d), q]
        return remote(block, block, z_send.at[side, d, j, q], z_recv.at[d, j, q],
                      jnp.clip(e + 1 - 2 * side, 0, n_ep - 1), t)

    def goes_right(j):
        return (j <= e) & (e < n_ep - 1)

    def goes_left(j):
        return (j >= e) & (e > 0)

    def z_onward(d, j, q):
        @pl.when(goes_right(j))
        def _():
            z_copy(0, d, j, q).start()

        @pl.when(goes_left(j))
        def _():
            z_copy(1, d, j, q).start()

    def spread(k, q):
        j = block_at(k)
        g = j * pieces + q

        @pl.when(k > 0)
        def _():
            z_copy(0, 0, j, q).wait_recv()

        z_onward(0, j, q)

        @pl.when(crosses(j))
        def _():
            for d in range(1, n_x):
                cross(tok_slot(j, q), g, d, t).start()

        across(tok_slot(j, q), g, 0, t).start()

    def forward(k, q):
        j = block_at(k)
        g = j * pieces + q
        for d in range(1, n_x):

            @pl.when(crosses(j))
            def _():
                cross(tok_slot(j, q), g, d, from_x(d)).wait_recv()

            @pl.when(~crosses(j))
            def _():
                z_copy(0, d, j, q).wait_recv()

            @pl.when(at_end(j))
            def _():
                z_onward(d, j, q)

            across(tok_slot(j, q), g, d, from_x(d)).start()

    piece = rows // CHUNKS

    def hop(j, c):
        at = pl.ds(pl.multiple_of(c * piece, 16), piece)
        after = jnp.clip(jnp.where(j > e, e + 1, e - 1), 0, n_ep - 1)
        slot = jnp.where((j < e) & (after == j), n_ep, j)
        return remote(res.at[j, at], pin.at[slot, at], r_send.at[j, c], r_recv.at[slot, c], after, t)

    def hop_arrives(slot, c):
        at = pl.ds(pl.multiple_of(c * piece, 16), piece)
        remote(res.at[0, at], pin.at[slot, at], r_send.at[0, c], r_recv.at[slot, c],
               jnp.clip(e + 1, 0, n_ep - 1), t).wait_recv()

    inner = (e > 0) & (e < n_ep - 1)

    def weights_to(d):
        return remote(wts.at[e], wts.at[e], w_send.at[d - 1], w_recv.at[e], (e + d) % n_ep, t)

    def weight_column(j):
        held = wts[j]
        mine = jnp.where(lax.broadcasted_iota(jnp.int32, held.shape, 0) == e, held, 0.0)
        line = jnp.sum(mine, axis=0, keepdims=True)
        shape = (rows, held.shape[1])
        same = lax.broadcasted_iota(jnp.int32, shape, 0) == lax.broadcasted_iota(jnp.int32, shape, 1)
        return jnp.sum(jnp.where(same, line, 0.0), axis=1, keepdims=True)

    loads["ei"].wait()
    loads["ng"].wait()

    def norm_rows(r, _):
        at = pl.ds(pl.multiple_of(r * PIECE, PIECE), PIECE)
        widened = ei[at, :].astype(jnp.float32)
        centred = widened - jnp.mean(widened, axis=-1, keepdims=True)
        spread_of = jnp.mean(centred * centred, axis=-1, keepdims=True)
        normed = centred * lax.rsqrt(spread_of + norm_floor) * ng[...]
        tok[e, t, r] = normed.astype(jnp.bfloat16)
        return 0

    lax.fori_loop(0, pieces, norm_rows, 0)
    pl.semaphore_wait(barrier, len(greeted))
    for q in range(pieces):
        spread(0, q)

    place = lax.broadcasted_iota(jnp.int32, (wts.shape[1], rows), 0)
    dense = jnp.zeros(place.shape, jnp.float32)
    for k in range(ids.shape[0]):
        dense += jnp.where(ids[k : k + 1, :] == place, rw[k : k + 1, :], 0.0)
    wts[e] = jnp.zeros(wts.shape[1:], jnp.float32)
    wts[e, :, 0:rows] = dense
    for d in range(1, n_ep):
        weights_to(d).start()

    loads["ig"].wait()
    loads["va"].wait()

    def gate_cols(c, _):
        at = pl.ds(pl.multiple_of(c * 128, 128), 128)
        gated[:, at] = (ig[:, at].astype(jnp.float32) * va[:, at].astype(jnp.float32)).astype(
            jnp.bfloat16
        )
        return 0

    lax.fori_loop(0, chans // 128, gate_cols, 0)

    def halo_copy():
        return remote(gated.at[pl.ds(rows - 16, 16)], halo, h_sem.at[0], h_sem.at[1],
                      jnp.minimum(e + 1, n_ep - 1), t)

    @pl.when(e < n_ep - 1)
    def _():
        halo_copy().start()

    loads["og"].wait()
    loads["taps"].wait()

    @pl.when(e == 0)
    def _():
        halo[...] = jnp.zeros_like(halo)

    @pl.when(e > 0)
    def _():
        halo_copy().wait_recv()

    def mix_cols(c, _):
        at = pl.ds(pl.multiple_of(c * 128, 128), 128)
        now = gated[:, at].astype(jnp.float32)
        before = halo[:, at].astype(jnp.float32)
        place = lax.broadcasted_iota(jnp.int32, now.shape, 0)
        one = jnp.where(place == 0, before[15:16], pltpu.roll(now, 1, 0))
        two = jnp.where(
            place == 0, before[14:15], jnp.where(place == 1, before[15:16], pltpu.roll(now, 2, 0))
        )
        state = taps[0:1, at] * two + taps[1:2, at] * one + taps[2:3, at] * now
        mixed[t, :, at] = (og[:, at].astype(jnp.float32) * state).astype(jnp.bfloat16)
        return 0

    lax.fori_loop(0, chans // 128, mix_cols, 0)
    for name in ("gw", "uw", "sg", "su"):
        loads[name].wait()

    def leave(k, _):
        j = block_at(k)
        gather_forward(hid_slot(j), first_hidden + j)
        gather_finish(hid_slot(j), first_hidden + j)
        part = hid.shape[-1]

        @pl.when(j != e)
        def _():
            remote(wts.at[e], wts.at[j], w_send.at[0], w_recv.at[j], j, t).wait_recv()

        weight = weight_column(j)
        for c in range(chans // TILE):
            at = slice(c * TILE, (c + 1) * TILE)
            total = dot32(hid[j, 0], dw[0:part, at])
            for lane in range(1, n_tp):
                total += dot32(hid[j, lane], dw[lane * part : (lane + 1) * part, at])
            res[j, :, at] = (weight * total).astype(jnp.bfloat16)

        @pl.when((j != e) & ~inner)
        def _():
            for c in range(CHUNKS):
                hop(j, c).start()
        return 0

    def meet(k):
        j = block_at(k)
        for q in range(pieces):
            gather_finish(tok_slot(j, q), j * pieces + q)
        block = tok[j].reshape(rows, width)
        hid[j, t] = silu_product(dot32(block, gw[...]), dot32(block, uw[...]))
        gather_start(hid_slot(j), first_hidden + j)

        @pl.when(k == 0)
        def _():
            block = tok[e].reshape(rows, width)
            shd[t] = silu_product(dot32(block, sg[...]), dot32(block, su[...]))
            gather_start(shd_slot, shared_g)
            loads["dw"].wait()

        @pl.when(k == n_ep - 1)
        def _():
            gather_start(mixed_slot, mixed_g)

    def step(s, _):
        for q in range(pieces):

            @pl.when(s + 1 < n_ep)
            def _():
                spread(s + 1, q)

            @pl.when(s < n_ep)
            def _():
                forward(s, q)

        @pl.when(~inner)
        def _():
            lax.fori_loop(jnp.maximum(s - 1, 0), s, leave, 0)

        k = jnp.where(inner, s - 1, s)

        @pl.when((k >= 0) & (k < n_ep))
        def _():
            meet(k)

        @pl.when(inner & (s == n_ep))
        def _():
            lax.fori_loop(0, n_ep, leave, 0)

        return 0

    lax.fori_loop(0, n_ep + 1, step, 0)

    gather_forward(shd_slot, shared_g)

    for phase in range(2):
        right = left_short if phase == 0 else ~left_short

        def relay(d, _):
            j = jnp.where(right, e + d, e - d)

            @pl.when(inner & (j >= 0) & (j < n_ep))
            def _():
                def relay_piece(c, _):
                    at = pl.ds(pl.multiple_of(c * piece, 16), piece)
                    hop_arrives(j, c)
                    total = res[j, at, :].astype(jnp.float32) + pin[j, at, :].astype(jnp.float32)
                    res[j, at, :] = total.astype(jnp.bfloat16)
                    hop(j, c).start()
                    return 0

                lax.fori_loop(0, CHUNKS, relay_piece, 0)

            return 0

        lax.fori_loop(1, n_ep, relay, 0)

    gather_forward(mixed_slot, mixed_g)
    gather_finish(shd_slot, shared_g)
    loads["sd"].wait()
    loads["mw"].wait()
    gather_finish(mixed_slot, mixed_g)

    def mixer_cols(c, _):
        at = pl.ds(pl.multiple_of(c * TILE, TILE), TILE)
        total = dot32(mixed[0], mw[0:chans, at])
        for lane in range(1, n_tp):
            total += dot32(mixed[lane], mw[lane * chans : (lane + 1) * chans, at])
        mix_out[:, at] = total.astype(jnp.bfloat16)
        return 0

    lax.fori_loop(0, chans // TILE, mixer_cols, 0)

    for here, slot in ((e > 0, e), (e < n_ep - 1, n_ep)):

        @pl.when(here)
        def _():
            for c in range(CHUNKS):
                hop_arrives(slot, c)

        @pl.when(~here)
        def _():
            pin[slot] = jnp.zeros(pin.shape[1:], pin.dtype)

    def combine_cols(c, _):
        at = pl.ds(pl.multiple_of(c * TILE, TILE), TILE)
        part = shd.shape[-1]
        total = dot32(shd[0], sd[0:part, at])
        for lane in range(1, n_tp):
            total += dot32(shd[lane], sd[lane * part : (lane + 1) * part, at])
        for found in (res[e, :, at], pin[e, :, at], pin[n_ep, :, at]):
            total += found.astype(jnp.float32)
        exp_out[:, at] = total.astype(jnp.bfloat16)
        return 0

    lax.fori_loop(0, chans // TILE, combine_cols, 0)

    @pl.when(e < n_ep - 1)
    def _():
        halo_copy().wait_send()

    def drain(j, _):
        def drain_z(d, q):
            @pl.when(goes_right(j))
            def _():
                z_copy(0, d, j, q).wait_send()

            @pl.when(goes_left(j))
            def _():
                z_copy(1, d, j, q).wait_send()

        for q in range(pieces):
            g = j * pieces + q
            drain_z(0, q)
            across(tok_slot(j, q), g, 0, t).wait_send()
            for d in range(1, n_x):

                @pl.when(crosses(j))
                def _():
                    cross(tok_slot(j, q), g, d, t).wait_send()

                @pl.when(at_end(j))
                def _():
                    drain_z(d, q)

                across(tok_slot(j, q), g, d, from_x(d)).wait_send()

        gather_drain(hid_slot(j), first_hidden + j)

        @pl.when(j != e)
        def _():
            for c in range(CHUNKS):
                hop(j, c).wait_send()

        return 0

    lax.fori_loop(0, n_ep, drain, 0)
    for d in range(1, n_ep):
        weights_to(d).wait_send()
    gather_drain(shd_slot, shared_g)
    gather_drain(mixed_slot, mixed_g)


def joined(n_ep, n_tp, *args):
    (og, ig, va, taps, mw, ei, ng, ids, rw, gw, uw, dw, sg, su, sd) = args
    gw, uw, dw, ng = gw[0], uw[0], dw[0], ng[None]
    bf, f32 = jnp.bfloat16, jnp.float32
    rows, chans = og.shape
    lane_rows, width = ei.shape
    n_x = n_tp // CORES
    pieces = lane_rows // PIECE
    sems = n_ep * pieces + n_ep + 2
    big = (og, ig, va, taps, mw, ei, ng, gw, uw, dw, sg, su, sd)
    out = jax.ShapeDtypeStruct((rows, chans), bf)
    vmem = pl.BlockSpec(memory_space=pltpu.VMEM)
    dma = pltpu.SemaphoreType.DMA
    return pl.pallas_call(
        functools.partial(kernel, n_ep, n_tp),
        out_shape=(out, out),
        in_specs=[vmem, vmem] + [pl.BlockSpec(memory_space=pl.ANY)] * len(big),
        out_specs=(vmem, vmem),
        scratch_shapes=[pltpu.VMEM(a.shape, a.dtype) for a in big]
        + [
            pltpu.VMEM((n_ep, n_tp, pieces, PIECE, width), bf),
            pltpu.VMEM((n_ep, n_tp, rows, gw.shape[-1]), bf),
            pltpu.VMEM((n_tp, rows, sg.shape[-1]), bf),
            pltpu.VMEM((n_tp, rows, chans), bf),
            pltpu.VMEM((rows, chans), bf),
            pltpu.VMEM((16, chans), bf),
            pltpu.VMEM((n_ep, rows, chans), bf),
            pltpu.VMEM((n_ep + 1, rows, chans), bf),
            pltpu.VMEM((n_ep, -(-n_ep // 8) * 8, -(-rows // 128) * 128), f32),
            dma((len(big),)),
            dma((2, n_x, n_ep, pieces)),
            dma((n_x, n_ep, pieces)),
            dma((sems, max(1, n_x - 1))),
            dma((sems, max(1, n_x - 1))),
            dma((sems, n_x)),
            dma((sems, n_x)),
            dma((n_ep, CHUNKS)),
            dma((n_ep + 1, CHUNKS)),
            dma((n_ep,)),
            dma((n_ep,)),
            dma((2,)),
        ],
        compiler_params=pltpu.CompilerParams(
            collective_id=0, has_side_effects=True, vmem_limit_bytes=60 * 1024 * 1024
        ),
    )(ids.T, rw.T, *big)


def local(*args):
    n_ep, n_tp = lax.axis_size("ep"), lax.axis_size("tp")
    chans, lane_rows = args[0].shape[1], args[5].shape[0]
    aligned = (
        n_tp % CORES == 0
        and lane_rows % PIECE == 0
        and lane_rows * n_tp == args[0].shape[0]
        and chans % TILE == 0
        and args[0].shape[0] % (16 * CHUNKS) == 0
        and args[9].shape[2] % 128 == 0
        and args[12].shape[1] % 128 == 0
    )
    return joined(n_ep, n_tp, *args) if aligned else plain(*args)


def solution(mesh):
    placed = (
        P(("grp", "ep"), "tp"),
        P(("grp", "ep"), "tp"),
        P(("grp", "ep"), "tp"),
        P(None, "tp"),
        P(None, "tp"),
        P(("grp", "ep", "tp"), None),
        P(),
        P(("grp", "ep"), None),
        P(("grp", "ep"), None),
        P("ep", None, "tp"),
        P("ep", None, "tp"),
        P("ep", None, "tp"),
        P(None, "tp"),
        P(None, "tp"),
        P(None, "tp"),
    )
    return jax.shard_map(
        local,
        mesh=mesh,
        in_specs=placed,
        out_specs=(P(("grp", "ep"), "tp"), P(("grp", "ep"), "tp")),
        check_vma=False,
    )
```
